512 devices in a mesh: grp: 2 (over y), fs: 32 (over z), tp: 8 (over x, core).
Axes of the slice: x: 4, y: 2, z: 32, core: 2. Of those that a mesh axis runs over, the one named last changes fastest.
The devices are a block of a 4x8x32 slice.
Arguments:
- tokens: bfloat16 [8192, 2048], P(('grp', 'fs'), 'tp'), parts along dimension 0, may hold values from -340 to 340
- routes: int32 [8192, 2], P(('grp', 'fs')), parts along dimension 0, may hold values from 0 to 7, all different within a row; in each aligned block of 128 rows (0 to 127, 128 to 255, ...) at most 40 rows name the same one
- route_weights: float32 [8192, 2], P(('grp', 'fs')), parts along dimension 0, may hold values from 0.2 to 1
- norm_gain: float32 [2048], P('fs'), may hold values from 0.1 to 1.9
- gate_weight: float32 [8, 2048, 4096], P(None, 'fs', 'tp'), may hold values from -0.125 to 0.125
- up_weight: float32 [8, 2048, 4096], P(None, 'fs', 'tp'), may hold values from -0.125 to 0.125
- down_weight: float32 [8, 2048, 4096], P(None, 'fs', 'tp'), may hold values from -0.09375 to 0.09375
Outputs:
- gate_out: bfloat16 [32, 4096, 1024], P('fs', 'grp', 'tp'), parts along dimension 1
- up_out: bfloat16 [32, 4096, 1024], P('fs', 'grp', 'tp'), parts along dimension 1
- down_out: bfloat16 [32, 4096, 1024], P('fs', 'grp', 'tp'), parts along dimension 1
- mixed_out: bfloat16 [8192, 2048], P(('grp', 'fs'), 'tp'), parts along dimension 0
The draws below stay inside these ranges and needn't reach their ends.
There are 2 independent parts, one for each index of `grp`. The reference program is written for one: setup_inputs(seed, part) draws one part's arguments, and reference() takes and returns one part's arrays. A program takes and returns all parts, laid end to end along the dimension named above; an argument that names none is the same for every part. Nothing has to cross between parts.
Inputs may be any that keep to these rules, and one draw needn't show every extreme that they name: `routes`: each row names 2 different experts; in each aligned block of 128 rows no expert is named by more than 40 rows, and in some block one expert is named by exactly 40 rows.
All inputs are finite; a program needn't handle non-finite values.
Results may differ from the reference program's by a relative error of at most 0.015.
Values may be sent and summed in bfloat16 or wider, within the bound.
No kernel may reach another device: no remote copies, remote signals or barrier semaphores. Data moves between devices by JAX's collectives and lax.ppermute only.
A program may use at most 64 MiB of HBM per device.

```python
import math
import jax
import jax.numpy as jnp
import numpy as np
from jax import lax

D = 2048
FF = 4096
EXPERTS = 8
TOP = 2
TOK_FS = 128
CAP = 40
SUB = 4
FFS = 128
TOKENS = 4096
N_FS = 32
N_TP = 8


def draw_tokens(key, part):
    noise_key, column_key, row_key = jax.random.split(key, 3)
    columns = jnp.arange(D, dtype=jnp.float32) / D
    column_scale = jnp.exp(math.log(4.0) * columns) * jax.random.uniform(column_key, (D,), jnp.float32, 0.6, 1.4)
    row_scale = jnp.exp(jax.random.uniform(row_key, (TOKENS, 1), jnp.float32, 0.0, math.log(10.0)))
    values = jnp.clip(jax.random.normal(noise_key, (TOKENS, D), jnp.float32), -6.0, 6.0)
    return (values * column_scale[None, :] * row_scale).astype(jnp.bfloat16)


def block_levels(stream_key, extent, cuts, least, top_value):
    loudness, own = 1.0, jax.random.fold_in(stream_key, 6)
    for axis_at, shards_of in cuts:
        steps = jnp.exp(jax.random.uniform(jax.random.fold_in(own, axis_at), (shards_of,), jnp.float32, least / len(cuts), top_value / len(cuts)))
        loudness = loudness * jnp.repeat(steps, extent[axis_at] // shards_of).reshape([-1 if axis == axis_at else 1 for axis in range(len(extent))])
    return loudness


def assign_block(own_key, own, number, rows, count, top, limit, skew):
    order = jax.random.permutation(own_key, count)
    crowded, ordinary = shares(count, rows * top, limit, skew, True), shares(count, rows * top, limit, skew, False)
    places = jnp.arange(count)

    def named(sizes, rotation):
        used = int((sizes > 0).sum())
        fixed = max(1, used // 4)
        shifted = fixed + (places - fixed + rotation * (used - fixed)) % max(1, count - fixed)
        return jnp.zeros((count,), jnp.int32).at[order[jnp.where(places < fixed, places, shifted)]].set(jnp.asarray(sizes, jnp.int32))

    sizes = jnp.where(number % 4 == 0, named(crowded, number // 4), named(ordinary, number - number // 4 - 1))
    mixed = jax.random.permutation(jax.random.fold_in(own, 3), count)
    donor, taker = mixed[0:count // 2 * 2:2], mixed[1:count // 2 * 2:2]
    slack = jnp.minimum(sizes[donor] - 1, limit - sizes[taker]) // 2
    slack = jnp.where((donor == order[0]) | (taker == order[0]) | (sizes[taker] == 0), 0, jnp.maximum(slack, 0))
    shifted = jax.random.randint(jax.random.fold_in(own, 4), (count // 2,), 0, 1 << 20) % (slack + 1)
    sizes = sizes.at[donor].add(-shifted).at[taker].add(shifted)
    members = jnp.searchsorted(jnp.cumsum(sizes), jnp.arange(rows * top), side="right").astype(jnp.int32)
    table = members.reshape(top, rows).T
    table = table[jax.random.permutation(jax.random.fold_in(own, 1), rows)]
    rotation = jax.random.randint(jax.random.fold_in(own, 2), (rows, 1), 0, top)
    return jnp.take_along_axis(table, (jnp.arange(top)[None, :] + rotation) % top, axis=1)


def shares(count, total, reach, skew, full):
    portions = [(1 << 20) // math.isqrt(rank ** skew) + 1 for rank in range(1, count + 1)]
    largest = reach if full else min(reach, max(-(-total // count), total * portions[0] // sum(portions)))
    least = 1 if total - largest >= count - 1 else 0
    holding, spare = [largest] + [least] * (count - 1), total - largest - least * (count - 1)
    while spare > 0:
        free = [i for i in range(1, count) if holding[i] < largest] or [i for i in range(1, count) if holding[i] < reach]
        mass, budget = sum([portions[i] for i in free]), spare
        for i in free:
            addition = min(reach - holding[i], max(1, budget * portions[i] // mass), spare)
            holding[i] = holding[i] + addition
            spare = spare - addition
    return np.array(holding)


def scatter_about(own_key, dims, scale, reach, cuts=(), kind=jnp.bfloat16):
    result = scale * jax.random.normal(own_key, dims, jnp.float32)
    if cuts:
        result = result * block_levels(own_key, dims, cuts, -0.22, 0.18)
    return jnp.clip(result, -reach, reach).astype(kind)


def setup_inputs(seed: int = 0, part: int = 0) -> dict:
    seeds = jax.random.split(jax.random.key(seed), 8)
    own_keys = jax.random.split(jax.random.fold_in(seeds[7], part), 8)
    tokens = draw_tokens(jax.random.fold_in(jax.random.fold_in(seeds[7], part), 71), part)
    routes_keys = jax.random.split(jax.random.fold_in(own_keys[1], 1), TOKENS // TOK_FS)
    routes_turns = jax.random.permutation(jax.random.fold_in(own_keys[1], 3), TOKENS // TOK_FS)
    routes = jax.vmap(lambda own, number: assign_block(jax.random.fold_in(own_keys[1], 2), own, number, TOK_FS, EXPERTS, TOP, CAP, 1))(routes_keys, routes_turns).reshape((TOKENS, TOP))
    route_weights = jnp.clip(0.2 + 0.8 * jax.random.uniform(own_keys[2], (TOKENS, TOP), jnp.float32) ** block_levels(own_keys[2], (TOKENS, TOP), ((0, 32),), -0.2, 0.2), 0.2, 1.0)
    norm_gain = jnp.clip(1.0 + 0.18 * jax.random.normal(seeds[3], (D,), jnp.float32), 0.1, 1.9)
    gate_weight = scatter_about(seeds[4], (EXPERTS, D, FF), D ** -0.5, 0.125, ((1, 32), (2, 8)), jnp.float32)
    up_weight = scatter_about(seeds[5], (EXPERTS, D, FF), D ** -0.5, 0.125, ((1, 32), (2, 8)), jnp.float32)
    down_weight = scatter_about(seeds[6], (EXPERTS, D, FF), FF ** -0.5, 0.09375, ((1, 32), (2, 8)), jnp.float32)
    return {"tokens": tokens, "routes": routes, "route_weights": route_weights, "norm_gain": norm_gain, "gate_weight": gate_weight, "up_weight": up_weight, "down_weight": down_weight}


epsilon = 1e-06

def relayout(matrix):
    blocked = matrix.reshape(EXPERTS, D, N_TP, SUB, FFS)
    return jnp.transpose(blocked, (0, 3, 1, 2, 4)).reshape(EXPERTS * SUB, D, N_TP * FFS)

def slot_table(routes):
    blocks = routes.reshape(N_FS, TOK_FS * TOP)
    onehot = (blocks[:, :, None] == jnp.arange(EXPERTS, dtype=jnp.int32)[None, None, :]).astype(jnp.int32)
    earlier = jnp.cumsum(onehot, axis=1) - onehot
    position = lax.optimization_barrier(jnp.sum(earlier * onehot, axis=2))
    block_index = jnp.arange(N_FS, dtype=jnp.int32)[:, None]
    return (block_index * CAP + position).astype(jnp.int32).reshape(TOKENS, TOP)

def reference(tokens, routes, route_weights, norm_gain, gate_weight, up_weight, down_weight):
    gain_row = norm_gain[None, :, None]
    gate_fold = (gain_row * gate_weight).astype(jnp.bfloat16)
    up_fold = (gain_row * up_weight).astype(jnp.bfloat16)
    down_cast = down_weight.astype(jnp.bfloat16)
    widened = tokens.astype(jnp.float32)
    row_scale = lax.rsqrt(lax.optimization_barrier(jnp.mean(widened * widened, axis=1, keepdims=True)) + epsilon)
    normed = (widened * row_scale).astype(jnp.bfloat16)
    slot_place = slot_table(routes)
    token_ids = jnp.broadcast_to(jnp.arange(TOKENS, dtype=jnp.int32)[:, None], (TOKENS, TOP))
    owner_rows = jnp.zeros((EXPERTS, N_FS * CAP), jnp.int32).at[routes, slot_place].set(token_ids)

    def one_expert(expert_args):
        gate_expert, up_expert, down_expert, owner_expert = expert_args
        token_rows = normed[owner_expert]
        gate_sums = jnp.dot(token_rows, gate_expert, preferred_element_type=jnp.float32)
        up_sums = jnp.dot(token_rows, up_expert, preferred_element_type=jnp.float32)
        hidden = (jax.nn.silu(gate_sums) * up_sums).astype(jnp.bfloat16)
        blocks = hidden.reshape(N_FS * CAP, SUB * N_TP, FFS).astype(jnp.float32)
        down_blocks = down_expert.reshape(D, SUB * N_TP, FFS).astype(jnp.float32)
        partial_value = jnp.einsum('mbf,dbf->bmd', blocks, down_blocks).astype(jnp.bfloat16)
        return lax.optimization_barrier(jnp.sum(partial_value.astype(jnp.float32), axis=0))
    results = lax.map(one_expert, (gate_fold, up_fold, down_cast, owner_rows))
    selected = results[routes, slot_place]
    mixed_rows = lax.optimization_barrier(jnp.sum(route_weights[:, :, None] * selected, axis=1)).astype(jnp.bfloat16)
    return (relayout(gate_fold), relayout(up_fold), relayout(down_cast), mixed_rows)
```

```python
import functools

import jax
import jax.numpy as jnp
from jax import lax
from jax.experimental import pallas as pl
from jax.experimental.pallas import tpu as pltpu
from jax.sharding import Mesh
from jax.sharding import PartitionSpec as P

FS = ("fs_hi", "fs_lo")
TP = ("tp_x", "tp_c")

epsilon = 1e-06


def shifted(value, axis, step):
    count = lax.axis_size(axis)
    return lax.ppermute(value, axis, [(k, (k + step) % count) for k in range(count)])


def exchange(value, axis):
    return lax.all_to_all(value, axis, split_axis=0, concat_axis=0, tiled=True)


def pack_kernel(turn, gain, gate, up, down, out):
    copies, _, width = out.shape
    width = width // 3
    factor = gain[...]
    for k, (source, scaled) in enumerate(((gate, True), (up, True), (down, False))):
        value = source[0]
        value = (factor * value if scaled else value).astype(jnp.bfloat16)
        for s in range(copies):
            out[s, :, k * width : (k + 1) * width] = value[:, s * width : (s + 1) * width]


def packed_weights(norm_gain, gate_weight, up_weight, down_weight, copies):
    experts, rows, columns = gate_weight.shape
    groups = lax.axis_size("grp")
    part = rows // groups
    width = columns // copies
    turn = lax.axis_index("grp").astype(jnp.int32).reshape(1)
    block = pl.BlockSpec((1, part, columns), lambda e, turn: (e, turn[0], 0))
    return pl.pallas_call(
        pack_kernel,
        out_shape=jax.ShapeDtypeStruct((experts * copies, part, 3 * width), jnp.bfloat16),
        grid_spec=pltpu.PrefetchScalarGridSpec(
            num_scalar_prefetch=1,
            grid=(experts,),
            in_specs=[
                pl.BlockSpec((part, 1), lambda e, turn: (turn[0], 0)),
                block,
                block,
                block,
            ],
            out_specs=pl.BlockSpec((copies, part, 3 * width), lambda e, turn: (e, 0, 0)),
        ),
        name="pack",
    )(turn, norm_gain.reshape(rows, 1), gate_weight, up_weight, down_weight)


def expert_kernel(place, own, other, *refs):
    parts, out = refs[:-1], refs[-1]
    count = len(parts)
    halves, tokens, cols = parts[0].shape[1:]
    width = own.shape[1] // 3
    sums = [jnp.zeros((tokens, 2 * width), jnp.float32) for _ in range(2)]
    for k, part in enumerate(parts):
        block = lax.rem(place[0] + (count - k), count) * halves
        for c in range(halves):
            rows = pl.ds(pl.multiple_of((block + c) * cols, cols), cols)
            left = part[0, c]
            sums = [
                total
                + jnp.dot(left, ref[rows, : 2 * width], preferred_element_type=jnp.float32)
                for total, ref in zip(sums, (own, other))
            ]
    hidden = []
    for total in sums:
        gate, up = total[:, :width], total[:, width:]
        hidden.append((gate / (1.0 + jnp.exp(-gate)) * up).astype(jnp.bfloat16))
    for k in range(count):
        for c in range(halves):
            start = (k * halves + c) * cols
            out[k, 0, c] = sum(
                lax.dot_general(
                    left,
                    ref[start : start + cols, 2 * width :],
                    (((1,), (1,)), ((), ())),
                    preferred_element_type=jnp.float32,
                )
                for left, ref in zip(hidden, (own, other))
            ).astype(jnp.bfloat16)


def expert_outputs(own, other, parts):
    copies, halves, tokens, cols = parts[0].shape
    place = lax.axis_index("tp_x").astype(jnp.int32).reshape(1)
    whole = pl.BlockSpec(own.shape, lambda t, place: (0, 0))
    return pl.pallas_call(
        expert_kernel,
        out_shape=jax.ShapeDtypeStruct((len(parts), *parts[0].shape), jnp.bfloat16),
        grid_spec=pltpu.PrefetchScalarGridSpec(
            num_scalar_prefetch=1,
            grid=(copies,),
            in_specs=[whole, whole]
            + [pl.BlockSpec((1, halves, tokens, cols), lambda t, place: (t, 0, 0, 0))]
            * len(parts),
            out_specs=pl.BlockSpec(
                (len(parts), 1, halves, tokens, cols), lambda t, place: (0, t, 0, 0, 0)
            ),
        ),
        compiler_params=pltpu.CompilerParams(vmem_limit_bytes=48 * 1024 * 1024),
        name="experts",
    )(place, own, other, *parts)


def expert_slots(routes, experts, capacity):
    flat_routes = routes.reshape(-1)
    onehot = (flat_routes[:, None] == jnp.arange(experts, dtype=jnp.int32)[None, :]).astype(
        jnp.int32
    )
    earlier = jnp.cumsum(onehot, axis=0) - onehot
    position = jnp.sum(earlier * onehot, axis=1)
    return (flat_routes * capacity + position).reshape(routes.shape)


def on_device(tokens, routes, route_weights, norm_gain, gate_weight, up_weight, down_weight):
    experts, rows, _ = gate_weight.shape
    copies = lax.axis_size("fs_lo")
    groups = lax.axis_size("grp")
    tp_count = lax.axis_size(TP)
    cores = lax.axis_size("tp_c")
    row_count, col_width = tokens.shape
    capacity = row_count * 5 // 16
    part = rows // groups

    packed = packed_weights(norm_gain, gate_weight, up_weight, down_weight, copies)
    mine = exchange(packed, FS)
    sources, _, triple = mine.shape
    weights = jnp.zeros((sources, groups, part, triple), jnp.bfloat16)
    for k in range(groups):
        piece = mine if k == 0 else shifted(mine, "grp", k)
        weights = lax.dynamic_update_slice_in_dim(
            weights, piece[:, None], lax.rem(lax.axis_index("grp") + groups - k, groups), axis=1
        )
    own = weights.reshape(sources * rows, triple)
    other = shifted(own, "tp_c", 1)

    widened = tokens.astype(jnp.float32)
    squares = lax.all_gather(jnp.sum(widened * widened, axis=1)[None], TP, tiled=True)
    row_scale = lax.rsqrt(
        jnp.sum(squares, axis=0)[:, None] / (col_width * tp_count) + epsilon
    )
    normed = (widened * row_scale).astype(jnp.bfloat16)

    slots = expert_slots(routes, experts, capacity)
    slot_ids = jnp.arange(experts * capacity, dtype=jnp.int32)
    select = jnp.any(slot_ids[:, None, None] == slots[None, :, :], axis=2).astype(jnp.bfloat16)
    outgoing = jnp.dot(select, normed, preferred_element_type=jnp.float32).astype(jnp.bfloat16)
    arrived = exchange(outgoing.reshape(experts, capacity, col_width), "fs_hi")
    share = experts * capacity // cores
    halved = exchange(arrived.reshape(cores, share, col_width), "tp_c")
    block = lax.all_gather(halved, "fs_lo")
    parts = [block] + [shifted(block, "tp_x", k) for k in range(1, lax.axis_size("tp_x"))]

    partial_value = expert_outputs(own, other, parts)
    over_x = jnp.sum(exchange(partial_value, "tp_x"), axis=0, dtype=jnp.float32)
    over_s = jnp.sum(
        exchange(over_x.astype(jnp.bfloat16), "fs_lo"), axis=0, dtype=jnp.float32
    )
    back = exchange(over_s.astype(jnp.bfloat16), "tp_c")
    returned = exchange(back.reshape(experts, capacity, col_width), "fs_hi")
    returned = returned.reshape(experts * capacity, col_width)
    combined = jnp.zeros((row_count, col_width), jnp.float32)
    for k in range(routes.shape[1]):
        chosen = (slots[:, k, None] == slot_ids[None, :]).astype(jnp.bfloat16)
        picked = jnp.dot(chosen, returned, preferred_element_type=jnp.float32)
        combined = combined + route_weights[:, k, None] * picked
    width = triple // 3
    outputs = [own[None, :, k * width : (k + 1) * width] for k in range(3)]
    return (*outputs, combined.astype(jnp.bfloat16))


def solution(mesh):
    split = Mesh(
        mesh.devices.reshape(mesh.shape["grp"], mesh.shape["fs"] // 4, 4, 4, 2),
        ("grp", *FS, *TP),
    )
    rows = P(("grp", *FS), None)
    weight = P(None, FS, TP)
    taken = P(FS, "grp", TP)
    return jax.shard_map(
        on_device,
        mesh=split,
        in_specs=(P(("grp", *FS), TP), rows, rows, P(FS), weight, weight, weight),
        out_specs=(taken, taken, taken, P(("grp", *FS), TP)),
        check_vma=False,
    )
```

```python
import jax
import jax.numpy as jnp
from jax import lax
from jax.experimental import pallas as pl
from jax.experimental.pallas import tpu as pltpu
from jax.sharding import Mesh
from jax.sharding import PartitionSpec as P

FS = ("fs_hi", "fs_lo")
TP = ("tp_x", "tp_c")

epsilon = 1e-06


def shifted(value, axis, step):
    count = lax.axis_size(axis)
    return lax.ppermute(value, axis, [(k, (k + step) % count) for k in range(count)])


def exchange(value, axis):
    return lax.all_to_all(value, axis, split_axis=0, concat_axis=0, tiled=True)


def pack_kernel(turn, gain, gate, up, down, out):
    copies, _, width = out.shape
    width = width // 3
    factor = gain[...]
    for k, (source, scaled) in enumerate(((gate, True), (up, True), (down, False))):
        value = source[0]
        value = (factor * value if scaled else value).astype(jnp.bfloat16)
        for s in range(copies):
            out[s, :, k * width : (k + 1) * width] = value[:, s * width : (s + 1) * width]


def packed_weights(norm_gain, gate_weight, up_weight, down_weight, copies):
    experts, rows, columns = gate_weight.shape
    groups = lax.axis_size("grp")
    part = rows // groups
    width = columns // copies
    turn = lax.axis_index("grp").astype(jnp.int32).reshape(1)
    block = pl.BlockSpec((1, part, columns), lambda e, turn: (e, turn[0], 0))
    return pl.pallas_call(
        pack_kernel,
        out_shape=jax.ShapeDtypeStruct((experts * copies, part, 3 * width), jnp.bfloat16),
        grid_spec=pltpu.PrefetchScalarGridSpec(
            num_scalar_prefetch=1,
            grid=(experts,),
            in_specs=[
                pl.BlockSpec((part, 1), lambda e, turn: (turn[0], 0)),
                block,
                block,
                block,
            ],
            out_specs=pl.BlockSpec((copies, part, 3 * width), lambda e, turn: (e, 0, 0)),
        ),
        name="pack",
    )(turn, norm_gain.reshape(rows, 1), gate_weight, up_weight, down_weight)


def expert_kernel(place, own, other, *refs):
    parts, out = refs[:-1], refs[-1]
    count = len(parts)
    halves, tokens, cols = parts[0].shape[1:]
    width = own.shape[1] // 3
    sums = [jnp.zeros((tokens, 2 * width), jnp.float32) for _ in range(2)]
    squares = jnp.zeros((tokens, cols), jnp.float32)
    for k, part in enumerate(parts):
        block = lax.rem(place[0] + (count - k), count) * halves
        for c in range(halves):
            start = (block + lax.rem(place[1] + (halves - c), halves)) * cols
            rows = pl.ds(pl.multiple_of(start, cols), cols)
            left = part[0, c]
            wide = left.astype(jnp.float32)
            squares = squares + wide * wide
            sums = [
                total
                + jnp.dot(left, ref[rows, : 2 * width], preferred_element_type=jnp.float32)
                for total, ref in zip(sums, (own, other))
            ]
    features = count * halves * cols
    row_scale = lax.rsqrt(jnp.sum(squares, axis=1, keepdims=True) / features + epsilon)
    hidden = []
    for total in sums:
        total = total * row_scale
        gate, up = total[:, :width], total[:, width:]
        hidden.append((gate / (1.0 + jnp.exp(-gate)) * up).astype(jnp.bfloat16))
    for k in range(count):
        for c in range(halves):
            start = (k * halves + c) * cols
            out[k, 0, c] = sum(
                lax.dot_general(
                    left,
                    ref[start : start + cols, 2 * width :],
                    (((1,), (1,)), ((), ())),
                    preferred_element_type=jnp.float32,
                )
                for left, ref in zip(hidden, (own, other))
            ).astype(jnp.bfloat16)


def expert_outputs(own, other, parts):
    copies, halves, tokens, cols = parts[0].shape
    place = jnp.stack([lax.axis_index("tp_x"), lax.axis_index("tp_c")]).astype(jnp.int32)
    whole = pl.BlockSpec(own.shape, lambda t, place: (0, 0))
    return pl.pallas_call(
        expert_kernel,
        out_shape=jax.ShapeDtypeStruct((len(parts), *parts[0].shape), jnp.bfloat16),
        grid_spec=pltpu.PrefetchScalarGridSpec(
            num_scalar_prefetch=1,
            grid=(copies,),
            in_specs=[whole, whole]
            + [pl.BlockSpec((1, halves, tokens, cols), lambda t, place: (t, 0, 0, 0))]
            * len(parts),
            out_specs=pl.BlockSpec(
                (len(parts), 1, halves, tokens, cols), lambda t, place: (0, t, 0, 0, 0)
            ),
        ),
        compiler_params=pltpu.CompilerParams(vmem_limit_bytes=48 * 1024 * 1024),
        name="experts",
    )(place, own, other, *parts)


def earlier_rows(named):
    count = named.shape[-1]
    before = jnp.arange(count)[:, None] < jnp.arange(count)[None, :]
    return jnp.dot(
        named.astype(jnp.bfloat16),
        before.astype(jnp.bfloat16),
        preferred_element_type=jnp.float32,
    ).astype(jnp.int32)


def assembled_weights(mine, rows):
    sources, part, triple = mine.shape
    groups = lax.axis_size("grp")
    weights = jnp.zeros((sources, groups, part, triple), jnp.bfloat16)
    for k in range(groups):
        piece = mine if k == 0 else shifted(mine, "grp", k)
        weights = lax.dynamic_update_slice_in_dim(
            weights, piece[:, None], lax.rem(lax.axis_index("grp") + groups - k, groups), axis=1
        )
    return weights.reshape(sources * rows, triple)


def dispatched(tokens, routes, capacity):
    row_count, col_width = tokens.shape
    cores = lax.axis_size("tp_c")
    table = routes.T.astype(jnp.bfloat16).reshape(-1, col_width)
    table = jnp.pad(table, ((0, 16 - table.shape[0]), (0, 0)))
    gathered = lax.all_gather(jnp.concatenate([tokens, table]), "fs_hi")
    sources = gathered.shape[0]
    named = gathered[:, row_count:].reshape(sources, -1, row_count)[:, : routes.shape[1]]
    expert = lax.axis_index("fs_hi").astype(jnp.bfloat16)
    match = jnp.any(named == expert, axis=1)
    position = earlier_rows(match)
    slot = jnp.arange(capacity, dtype=jnp.int32)[None, :, None]
    select = ((position[:, None, :] == slot) & match[:, None, :]).astype(jnp.bfloat16)
    packed = jnp.einsum(
        "jpt,jtc->jpc", select, gathered[:, :row_count], preferred_element_type=jnp.float32
    ).astype(jnp.bfloat16)
    packed = packed.reshape(cores, sources * capacity // cores, col_width)
    core = lax.axis_index("tp_c")
    halves = []
    for j in range(cores):
        half = lax.dynamic_index_in_dim(
            packed, lax.rem(core + j, cores), axis=0, keepdims=False
        )
        halves.append(half if j == 0 else shifted(half, "tp_c", j))
    block = lax.all_gather(jnp.stack(halves), "fs_lo")
    return [block] + [
        shifted(block, "tp_x", k) for k in range(1, lax.axis_size("tp_x"))
    ]


def on_device(tokens, routes, route_weights, norm_gain, gate_weight, up_weight, down_weight):
    experts, rows, _ = gate_weight.shape
    copies = lax.axis_size("fs_lo")
    row_count, col_width = tokens.shape
    capacity = row_count * 5 // 16

    packed = packed_weights(norm_gain, gate_weight, up_weight, down_weight, copies)
    mine = exchange(packed, FS)
    parts = dispatched(tokens, routes, capacity)
    own = assembled_weights(mine, rows)
    other = shifted(own, "tp_c", 1)

    partial_value = expert_outputs(own, other, parts)
    over_x = jnp.sum(exchange(partial_value, "tp_x"), axis=0, dtype=jnp.float32)
    over_x = over_x.astype(jnp.bfloat16)
    sent = exchange(over_x.reshape(-1, *over_x.shape[2:]), ("fs_lo", "tp_c"))
    over_s = jnp.sum(sent.reshape(over_x.shape), axis=0, dtype=jnp.float32)
    returned = exchange(
        over_s.astype(jnp.bfloat16).reshape(experts, capacity, col_width), "fs_hi"
    ).reshape(experts * capacity, col_width)

    expert_ids = jnp.arange(experts, dtype=jnp.int32)
    onehot = [expert_ids[:, None] == routes[None, :, k] for k in range(routes.shape[1])]
    position = earlier_rows(sum(hot.astype(jnp.int32) for hot in onehot))
    slot_ids = jnp.arange(experts * capacity, dtype=jnp.int32)
    combined = jnp.zeros((row_count, col_width), jnp.float32)
    for k, hot in enumerate(onehot):
        slot = jnp.sum(jnp.where(hot, expert_ids[:, None] * capacity + position, 0), axis=0)
        chosen = (slot[:, None] == slot_ids[None, :]).astype(jnp.bfloat16)
        picked = jnp.dot(chosen, returned, preferred_element_type=jnp.float32)
        combined = combined + route_weights[:, k, None] * picked
    width = own.shape[1] // 3
    outputs = [own[None, :, k * width : (k + 1) * width] for k in range(3)]
    return (*outputs, combined.astype(jnp.bfloat16))


def solution(mesh):
    split = Mesh(
        mesh.devices.reshape(mesh.shape["grp"], mesh.shape["fs"] // 4, 4, 4, 2),
        ("grp", *FS, *TP),
    )
    rows = P(("grp", *FS), None)
    weight = P(None, FS, TP)
    taken = P(FS, "grp", TP)
    return jax.shard_map(
        on_device,
        mesh=split,
        in_specs=(P(("grp", *FS), TP), rows, rows, P(FS), weight, weight, weight),
        out_specs=(taken, taken, taken, P(("grp", *FS), TP)),
        check_vma=False,
    )
```

```python
import functools

import jax
import jax.numpy as jnp
from jax import lax
from jax.experimental import pallas as pl
from jax.experimental.pallas import tpu as pltpu
from jax.sharding import Mesh
from jax.sharding import PartitionSpec as P

FS = ("fs_hi", "fs_lo")
TP = ("tp_x", "tp_c")

epsilon = 1e-06
chunks = 2


def shifted(value, axis, step):
    count = lax.axis_size(axis)
    return lax.ppermute(value, axis, [(k, (k + step) % count) for k in range(count)])


def exchange(value, axis):
    return lax.all_to_all(value, axis, split_axis=0, concat_axis=0, tiled=True)


def position_of(*axes):
    return jnp.stack([lax.axis_index(axis) for axis in axes]).astype(jnp.int32)


def pack_kernel(turn, gain, gate, up, down, out):
    copies, part, width = out.shape
    width = width // 3
    rows = gain.shape[1]
    row = lax.broadcasted_iota(jnp.int32, (part, rows), 0) + turn[0] * part
    column = lax.broadcasted_iota(jnp.int32, (part, rows), 1)
    factor = jnp.sum(jnp.where(row == column, gain[...], 0.0), axis=1, keepdims=True)
    for k, (source, scaled) in enumerate(((gate, True), (up, True), (down, False))):
        value = source[0]
        value = (factor * value if scaled else value).astype(jnp.bfloat16)
        for s in range(copies):
            out[s, :, k * width : (k + 1) * width] = value[:, s * width : (s + 1) * width]


def packed_weights(norm_gain, gate_weight, up_weight, down_weight, copies):
    experts, rows, columns = gate_weight.shape
    part = rows // lax.axis_size("grp")
    width = columns // copies
    block = pl.BlockSpec((1, part, columns), lambda e, turn: (e, turn[0], 0))
    return pl.pallas_call(
        pack_kernel,
        out_shape=jax.ShapeDtypeStruct((experts * copies, part, 3 * width), jnp.bfloat16),
        grid_spec=pltpu.PrefetchScalarGridSpec(
            num_scalar_prefetch=1,
            grid=(experts,),
            in_specs=[pl.BlockSpec((1, rows), lambda e, turn: (0, 0)), block, block, block],
            out_specs=pl.BlockSpec((copies, part, 3 * width), lambda e, turn: (e, 0, 0)),
        ),
        name="pack",
    )(position_of("grp"), norm_gain.reshape(1, rows), gate_weight, up_weight, down_weight)


def before_matrix(count):
    row = lax.broadcasted_iota(jnp.int32, (count, count), 0)
    column = lax.broadcasted_iota(jnp.int32, (count, count), 1)
    return jnp.where(row < column, 1.0, 0.0).astype(jnp.bfloat16)


def dispatch_kernel(routes, tokens, out):
    experts, capacity, _ = out.shape
    top, count = routes.shape
    expert = lax.broadcasted_iota(jnp.int32, (experts, count), 0)
    named = routes[0:1, :] == expert
    for k in range(1, top):
        named = named | (routes[k : k + 1, :] == expert)
    position = jnp.dot(
        jnp.where(named, 1.0, 0.0).astype(jnp.bfloat16),
        before_matrix(count),
        preferred_element_type=jnp.float32,
    )
    position = jnp.where(named, position.astype(jnp.int32), capacity)
    slot = lax.broadcasted_iota(jnp.int32, (capacity, count), 0)
    for e in range(experts):
        select = jnp.where(position[e : e + 1, :] == slot, 1.0, 0.0).astype(jnp.bfloat16)
        out[e] = jnp.dot(
            select, tokens[...], preferred_element_type=jnp.float32
        ).astype(jnp.bfloat16)


def dispatched(tokens, routes, experts, capacity):
    return pl.pallas_call(
        dispatch_kernel,
        out_shape=jax.ShapeDtypeStruct((experts, capacity, tokens.shape[1]), jnp.bfloat16),
        name="dispatch",
    )(routes.T, tokens)


def expert_kernel(place, own, other, *refs):
    count = len(refs) // 2
    parts, outs = refs[:count], refs[count:]
    copies, halves, tokens, cols = parts[0].shape
    width = own.shape[1] // 3
    rows = copies * tokens
    sums = [jnp.zeros((rows, 2 * width), jnp.float32) for _ in range(2)]
    squares = jnp.zeros((rows, cols), jnp.float32)

    def block(k, c):
        start = lax.rem(place[0] + k, count) * halves + c
        return pl.ds(pl.multiple_of(start * cols, cols), cols)

    for k, part in enumerate(parts):
        for c in range(halves):
            core = lax.rem(place[1] + (halves - c), halves)
            left = part[:, c].reshape(rows, cols)
            wide = left.astype(jnp.float32)
            squares = squares + wide * wide
            where = block(count - k, core)
            sums = [
                total
                + jnp.dot(left, ref[where, : 2 * width], preferred_element_type=jnp.float32)
                for total, ref in zip(sums, (own, other))
            ]
    features = count * halves * cols
    row_scale = lax.rsqrt(jnp.sum(squares, axis=1, keepdims=True) / features + epsilon)
    hidden = []
    for total in sums:
        total = total * row_scale
        gate, up = total[:, :width], total[:, width:]
        hidden.append((gate / (1.0 + jnp.exp(-gate)) * up).astype(jnp.bfloat16))
    hidden = jnp.concatenate(hidden, axis=1)
    for k, out in enumerate(outs):
        for c in range(halves):
            where = block(k, c)
            down = jnp.concatenate([ref[where, 2 * width :] for ref in (own, other)], axis=1)
            value = lax.dot_general(
                hidden, down, (((1,), (1,)), ((), ())), preferred_element_type=jnp.float32
            ).astype(jnp.bfloat16)
            for r in range(copies):
                target = lax.rem(place[2] + (copies - r), copies)
                out[pl.ds(target, 1), c] = value[r * tokens : (r + 1) * tokens][None]


def expert_outputs(own, other, parts, chunk):
    copies, halves, tokens, cols = parts[0].shape
    share = tokens // chunks
    whole = pl.BlockSpec(own.shape, lambda t, place: (0, 0))
    piece = (copies, halves, share, cols)
    return pl.pallas_call(
        expert_kernel,
        out_shape=[jax.ShapeDtypeStruct(piece, jnp.bfloat16)] * len(parts),
        grid_spec=pltpu.PrefetchScalarGridSpec(
            num_scalar_prefetch=1,
            grid=(1,),
            in_specs=[whole, whole]
            + [pl.BlockSpec(piece, lambda t, place: (0, 0, chunk, 0))] * len(parts),
            out_specs=[pl.BlockSpec(piece, lambda t, place: (0, 0, 0, 0))] * len(parts),
        ),
        compiler_params=pltpu.CompilerParams(vmem_limit_bytes=48 * 1024 * 1024),
        name="experts",
    )(position_of("tp_x", "tp_c", "fs_lo"), own, other, *parts)


def combine_kernel(routes, route_weights, returned, out):
    experts, capacity, cols = returned.shape
    top, count = routes.shape
    expert = lax.broadcasted_iota(jnp.int32, (experts, count), 0)
    named = [routes[k : k + 1, :] == expert for k in range(top)]
    either = functools.reduce(jnp.logical_or, named)
    position = jnp.dot(
        jnp.where(either, 1.0, 0.0).astype(jnp.bfloat16),
        before_matrix(count),
        preferred_element_type=jnp.float32,
    ).astype(jnp.int32)
    values = returned[...].reshape(experts * capacity, cols)
    slot = lax.broadcasted_iota(jnp.int32, (experts * capacity, count), 0)
    total = jnp.zeros((count, cols), jnp.float32)
    for k in range(top):
        mine = jnp.sum(
            jnp.where(named[k], expert * capacity + position, 0), axis=0, keepdims=True
        )
        chosen = jnp.where(mine == slot, 1.0, 0.0).astype(jnp.bfloat16)
        picked = lax.dot_general(
            chosen, values, (((0,), (0,)), ((), ())), preferred_element_type=jnp.float32
        )
        total = total + route_weights[:, k : k + 1] * picked
    out[...] = total.astype(jnp.bfloat16)


def combined(routes, route_weights, returned):
    return pl.pallas_call(
        combine_kernel,
        out_shape=jax.ShapeDtypeStruct((routes.shape[0], returned.shape[2]), jnp.bfloat16),
        name="combine",
    )(routes.T, route_weights, returned)


def assembled_weights(mine, rows):
    sources, part, triple = mine.shape
    groups = lax.axis_size("grp")
    weights = jnp.zeros((sources, groups, part, triple), jnp.bfloat16)
    for k in range(groups):
        piece = mine if k == 0 else shifted(mine, "grp", k)
        weights = lax.dynamic_update_slice_in_dim(
            weights, piece[:, None], lax.rem(lax.axis_index("grp") + groups - k, groups), axis=1
        )
    return weights.reshape(sources * rows, triple)


def halved(arrived):
    experts, capacity, cols = arrived.shape
    cores = lax.axis_size("tp_c")
    arrived = arrived.reshape(cores, experts * capacity // cores, cols)
    halves = []
    for j in range(cores):
        half = lax.dynamic_index_in_dim(
            arrived, lax.rem(lax.axis_index("tp_c") + j, cores), axis=0, keepdims=False
        )
        halves.append(half if j == 0 else shifted(half, "tp_c", j))
    return jnp.stack(halves)


def on_device(tokens, routes, route_weights, norm_gain, gate_weight, up_weight, down_weight):
    experts, rows, _ = gate_weight.shape
    copies = lax.axis_size("fs_lo")
    row_count, col_width = tokens.shape
    capacity = row_count * 5 // 16

    outgoing = dispatched(tokens, routes, experts, capacity)
    arrived = exchange(outgoing, "fs_hi")
    block = lax.optimization_barrier(halved(arrived))
    blocks = [block] + [shifted(block, "fs_lo", k) for k in range(1, copies)]
    blocks = jnp.stack(blocks)
    parts = [blocks] + [
        shifted(blocks, "tp_x", k) for k in range(1, lax.axis_size("tp_x"))
    ]

    packed = packed_weights(norm_gain, gate_weight, up_weight, down_weight, copies)
    mine = exchange(packed, FS)
    own = assembled_weights(mine, rows)
    other = shifted(own, "tp_c", 1)

    sums = []
    for t in range(chunks):
        outs = expert_outputs(own, other, parts, t)
        got = [outs[0]] + [shifted(outs[k], "tp_x", k) for k in range(1, len(outs))]
        over_x = sum(value.astype(jnp.float32) for value in got).astype(jnp.bfloat16)
        sent = exchange(over_x.reshape(-1, *over_x.shape[2:]), ("fs_lo", "tp_c"))
        over_s = jnp.sum(sent.reshape(over_x.shape), axis=0, dtype=jnp.float32)
        sums.append(over_s.astype(jnp.bfloat16))
    back = jnp.concatenate(sums, axis=1).reshape(experts, capacity, col_width)
    returned = exchange(back, "fs_hi")
    width = own.shape[1] // 3
    outputs = [own[None, :, k * width : (k + 1) * width] for k in range(3)]
    return (*outputs, combined(routes, route_weights, returned))


def solution(mesh):
    split = Mesh(
        mesh.devices.reshape(mesh.shape["grp"], mesh.shape["fs"] // 4, 4, 4, 2),
        ("grp", *FS, *TP),
    )
    rows = P(("grp", *FS), None)
    weight = P(None, FS, TP)
    taken = P(FS, "grp", TP)

    return jax.shard_map(
        on_device,
        mesh=split,
        in_specs=(P(("grp", *FS), TP), rows, rows, P(FS), weight, weight, weight),
        out_specs=(taken, taken, taken, P(("grp", *FS), TP)),
        check_vma=False,
    )
```

```python
import functools

import jax
import jax.numpy as jnp
from jax import lax
from jax.experimental import pallas as pl
from jax.experimental.pallas import tpu as pltpu
from jax.sharding import Mesh
from jax.sharding import PartitionSpec as P

FS = ("fs_hi", "fs_lo")
TP = ("tp_x", "tp_c")

epsilon = 1e-06


def shifted(value, axis, step):
    count = lax.axis_size(axis)
    return lax.ppermute(value, axis, [(k, (k + step) % count) for k in range(count)])


def vmem(mebibytes):
    return pltpu.CompilerParams(vmem_limit_bytes=mebibytes * 1024 * 1024)


def exchange(value, axis):
    return lax.all_to_all(value, axis, split_axis=0, concat_axis=0, tiled=True)


def position_of(*axes):
    return jnp.stack([lax.axis_index(axis) for axis in axes]).astype(jnp.int32)


def pack_kernel(turn, gain, gate, up, down, out):
    copies, part, width = out.shape
    width = width // 3
    rows = gain.shape[1]
    row = lax.broadcasted_iota(jnp.int32, (part, rows), 0) + turn[0] * part
    column = lax.broadcasted_iota(jnp.int32, (part, rows), 1)
    factor = jnp.sum(jnp.where(row == column, gain[...], 0.0), axis=1, keepdims=True)
    for k, (source, scaled) in enumerate(((gate, True), (up, True), (down, False))):
        value = source[0]
        value = (factor * value if scaled else value).astype(jnp.bfloat16)
        for s in range(copies):
            out[s, :, k * width : (k + 1) * width] = value[:, s * width : (s + 1) * width]


def packed_weights(norm_gain, gate_weight, up_weight, down_weight, copies):
    experts, rows, columns = gate_weight.shape
    part = rows // lax.axis_size("grp")
    width = columns // copies
    block = pl.BlockSpec((1, part, columns), lambda e, turn: (e, turn[0], 0))
    return pl.pallas_call(
        pack_kernel,
        out_shape=jax.ShapeDtypeStruct((experts * copies, part, 3 * width), jnp.bfloat16),
        grid_spec=pltpu.PrefetchScalarGridSpec(
            num_scalar_prefetch=1,
            grid=(experts,),
            in_specs=[pl.BlockSpec((1, rows), lambda e, turn: (0, 0)), block, block, block],
            out_specs=pl.BlockSpec((copies, part, 3 * width), lambda e, turn: (e, 0, 0)),
        ),
        compiler_params=vmem(12),
        name="pack",
    )(position_of("grp"), norm_gain.reshape(1, rows), gate_weight, up_weight, down_weight)


def before_matrix(count):
    row = lax.broadcasted_iota(jnp.int32, (count, count), 0)
    column = lax.broadcasted_iota(jnp.int32, (count, count), 1)
    return jnp.where(row < column, 1.0, 0.0).astype(jnp.bfloat16)


def dispatch_kernel(routes, tokens, out):
    experts, capacity, _ = out.shape
    top, count = routes.shape
    expert = lax.broadcasted_iota(jnp.int32, (experts, count), 0)
    named = routes[0:1, :] == expert
    for k in range(1, top):
        named = named | (routes[k : k + 1, :] == expert)
    position = jnp.dot(
        jnp.where(named, 1.0, 0.0).astype(jnp.bfloat16),
        before_matrix(count),
        preferred_element_type=jnp.float32,
    )
    position = jnp.where(named, position.astype(jnp.int32), capacity)
    slot = lax.broadcasted_iota(jnp.int32, (capacity, count), 0)
    for e in range(experts):
        select = jnp.where(position[e : e + 1, :] == slot, 1.0, 0.0).astype(jnp.bfloat16)
        out[e] = jnp.dot(
            select, tokens[...], preferred_element_type=jnp.float32
        ).astype(jnp.bfloat16)


def dispatched(tokens, routes, experts, capacity):
    return pl.pallas_call(
        dispatch_kernel,
        out_shape=jax.ShapeDtypeStruct((experts, capacity, tokens.shape[1]), jnp.bfloat16),
        compiler_params=vmem(12),
        name="dispatch",
    )(routes.T, tokens)


def expert_kernel(span, count, place, *refs):
    first, share = span
    total, assembled = len(refs), refs[-2:]
    parts, outs = refs[total - 2 - 2 * count : total - 2 - count], refs[total - 2 - count : -2]
    pieces = refs[: total - 2 - 2 * count]
    groups = len(pieces) // 2
    copies, halves, _, cols = parts[0].shape
    part, width = pieces[0].shape[1], pieces[0].shape[2] // 3
    rows = copies * share
    for k in range(groups):
        index = lax.rem(place[3] + (groups - k), groups)
        for held, piece in zip(assembled, (pieces[k], pieces[groups + k])):
            held[:, pl.ds(index, 1)] = piece[...][:, None]

    def block(held, k, c, start, end):
        sources = cols // (groups * part)
        at = (lax.rem(place[0] + k, count) * halves + c) * sources
        return held[pl.ds(at, sources), :, :, start:end].reshape(cols, end - start)

    sums = [jnp.zeros((rows, 2 * width), jnp.float32) for _ in range(2)]
    squares = jnp.zeros((rows, cols), jnp.float32)
    for k in range(count):
        for c in range(halves):
            core = lax.rem(place[1] + (halves - c), halves)
            left = parts[k][:, c, first : first + share].reshape(rows, cols)
            wide = left.astype(jnp.float32)
            squares = squares + wide * wide
            sums = [
                value
                + jnp.dot(
                    left,
                    block(held, count - k, core, 0, 2 * width),
                    preferred_element_type=jnp.float32,
                )
                for value, held in zip(sums, assembled)
            ]
    features = count * halves * cols
    row_scale = lax.rsqrt(jnp.sum(squares, axis=1, keepdims=True) / features + epsilon)
    hidden = []
    for value in sums:
        value = value * row_scale
        gate, up = value[:, :width], value[:, width:]
        hidden.append((gate / (1.0 + jnp.exp(-gate)) * up).astype(jnp.bfloat16))
    hidden = jnp.concatenate(hidden, axis=1)
    for k, out in enumerate(outs):
        for c in range(halves):
            down = jnp.concatenate(
                [block(held, k, c, 2 * width, 3 * width) for held in assembled], axis=1
            )
            value = lax.dot_general(
                hidden, down, (((1,), (1,)), ((), ())), preferred_element_type=jnp.float32
            ).astype(jnp.bfloat16)
            for r in range(copies):
                target = lax.rem(place[2] + (copies - r), copies)
                out[pl.ds(target, 1), c] = value[r * share : (r + 1) * share][None]


def whole_block(value):
    return pl.BlockSpec(value.shape, lambda t, place, rank=len(value.shape): (0,) * rank)


def expert_outputs(pieces, parts, span):
    copies, halves, _, cols = parts[0].shape
    sources, part, triple = pieces[0].shape
    out = jax.ShapeDtypeStruct((copies, halves, span[1], cols), jnp.bfloat16)
    inputs = (*pieces, *parts)
    held = pltpu.VMEM((sources, len(pieces) // 2, part, triple), jnp.bfloat16)
    return pl.pallas_call(
        functools.partial(expert_kernel, span, len(parts)),
        out_shape=[out] * len(parts),
        grid_spec=pltpu.PrefetchScalarGridSpec(
            num_scalar_prefetch=1,
            grid=(1,),
            in_specs=[whole_block(value) for value in inputs],
            out_specs=[whole_block(out)] * len(parts),
            scratch_shapes=[held, held],
        ),
        compiler_params=vmem(32),
        name="experts",
    )(position_of("tp_x", "tp_c", "fs_lo", "grp"), *inputs)


def choose_kernel(routes, out):
    top, slots, count = out.shape
    capacity = count * 5 // 16
    expert = lax.broadcasted_iota(jnp.int32, (slots // capacity, count), 0)
    named = [routes[k : k + 1, :] == expert for k in range(top)]
    either = functools.reduce(jnp.logical_or, named)
    position = jnp.dot(
        jnp.where(either, 1.0, 0.0).astype(jnp.bfloat16),
        before_matrix(count),
        preferred_element_type=jnp.float32,
    ).astype(jnp.int32)
    slot = lax.broadcasted_iota(jnp.int32, (slots, count), 0)
    for k in range(top):
        mine = jnp.sum(
            jnp.where(named[k], expert * capacity + position, 0), axis=0, keepdims=True
        )
        out[k] = jnp.where(mine == slot, 1.0, 0.0).astype(jnp.bfloat16)


def chosen_slots(routes, slots):
    count, top = routes.shape
    return pl.pallas_call(
        choose_kernel,
        out_shape=jax.ShapeDtypeStruct((top, slots, count), jnp.bfloat16),
        compiler_params=vmem(12),
        name="choose",
    )(routes.T)


def combine_kernel(place, chosen, route_weights, returned, out):
    top, slots, _ = chosen.shape
    values = returned[...].reshape(slots, returned.shape[2])
    total = jnp.zeros(out.shape, jnp.float32)
    for k in range(top):
        picked = lax.dot_general(
            chosen[k], values, (((0,), (0,)), ((), ())), preferred_element_type=jnp.float32
        )
        total = total + route_weights[:, k : k + 1] * picked
    out[...] = total.astype(jnp.bfloat16)


def combined(chosen, route_weights, returned):
    out = jax.ShapeDtypeStruct((route_weights.shape[0], returned.shape[2]), jnp.bfloat16)
    inputs = (chosen, route_weights, returned)
    return pl.pallas_call(
        combine_kernel,
        out_shape=out,
        grid_spec=pltpu.PrefetchScalarGridSpec(
            num_scalar_prefetch=1,
            grid=(1,),
            in_specs=[whole_block(value) for value in inputs],
            out_specs=whole_block(out),
        ),
        compiler_params=vmem(12),
        name="combine",
    )(position_of("grp"), *inputs)


def assembled_weights(pieces, rows):
    groups = len(pieces)
    sources, part, triple = pieces[0].shape
    weights = jnp.zeros((sources, groups, part, triple), jnp.bfloat16)
    for k, piece in enumerate(pieces):
        weights = lax.dynamic_update_slice_in_dim(
            weights, piece[:, None], lax.rem(lax.axis_index("grp") + groups - k, groups), axis=1
        )
    return weights.reshape(sources * rows, triple)


def halved(arrived):
    experts, capacity, cols = arrived.shape
    cores = lax.axis_size("tp_c")
    arrived = arrived.reshape(cores, experts * capacity // cores, cols)
    halves = []
    for j in range(cores):
        half = lax.dynamic_index_in_dim(
            arrived, lax.rem(lax.axis_index("tp_c") + j, cores), axis=0, keepdims=False
        )
        halves.append(half if j == 0 else shifted(half, "tp_c", j))
    return jnp.stack(halves)


def on_device(tokens, routes, route_weights, norm_gain, gate_weight, up_weight, down_weight):
    experts, rows, _ = gate_weight.shape
    copies = lax.axis_size("fs_lo")
    row_count, col_width = tokens.shape
    capacity = row_count * 5 // 16
    share = experts * capacity // lax.axis_size("tp_c")
    cut = share * 5 // 8 // 32 * 32
    spans = ((0, cut), (cut, share - cut))

    outgoing = dispatched(tokens, routes, experts, capacity)
    arrived = exchange(outgoing, "fs_hi")
    block = lax.optimization_barrier(halved(arrived))
    blocks = [block] + [shifted(block, "fs_lo", k) for k in range(1, copies)]
    blocks = jnp.stack(blocks)
    parts = [blocks] + [
        shifted(blocks, "tp_x", k) for k in range(1, lax.axis_size("tp_x"))
    ]

    packed = packed_weights(norm_gain, gate_weight, up_weight, down_weight, copies)
    mine = exchange(packed, FS)
    own = [mine] + [shifted(mine, "grp", k) for k in range(1, lax.axis_size("grp"))]
    other = [shifted(piece, "tp_c", 1) for piece in own]
    chosen = chosen_slots(routes, experts * capacity)

    sums = []
    for span in spans:
        outs = expert_outputs(own + other, parts, span)
        got = [outs[0]] + [shifted(outs[k], "tp_x", k) for k in range(1, len(outs))]
        over_x = sum(value.astype(jnp.float32) for value in got).astype(jnp.bfloat16)
        sent = exchange(over_x.reshape(-1, *over_x.shape[2:]), ("fs_lo", "tp_c"))
        over_s = jnp.sum(sent.reshape(over_x.shape), axis=0, dtype=jnp.float32)
        sums.append(over_s.astype(jnp.bfloat16))
    own = assembled_weights(own, rows)
    back = jnp.concatenate(sums, axis=1).reshape(experts, capacity, col_width)
    returned = exchange(back, "fs_hi")
    width = own.shape[1] // 3
    outputs = [own[None, :, k * width : (k + 1) * width] for k in range(3)]
    return (*outputs, combined(chosen, route_weights, returned))


def solution(mesh):
    split = Mesh(
        mesh.devices.reshape(mesh.shape["grp"], mesh.shape["fs"] // 4, 4, 4, 2),
        ("grp", *FS, *TP),
    )
    rows = P(("grp", *FS), None)
    weight = P(None, FS, TP)
    taken = P(FS, "grp", TP)

    return jax.shard_map(
        on_device,
        mesh=split,
        in_specs=(P(("grp", *FS), TP), rows, rows, P(FS), weight, weight, weight),
        out_specs=(taken, taken, taken, P(("grp", *FS), TP)),
        check_vma=False,
    )
```

```python
import functools

import jax
import jax.numpy as jnp
from jax import lax
from jax.experimental import pallas as pl
from jax.experimental.pallas import tpu as pltpu
from jax.sharding import Mesh
from jax.sharding import PartitionSpec as P

FS = ("fs_hi", "fs_lo")
TP = ("tp_x", "tp_c")

epsilon = 1e-06


def shifted(value, axis, step):
    count = lax.axis_size(axis)
    return lax.ppermute(value, axis, [(k, (k + step) % count) for k in range(count)])


def vmem(mebibytes):
    return pltpu.CompilerParams(vmem_limit_bytes=mebibytes * 1024 * 1024)


def exchange(value, axis):
    return lax.all_to_all(value, axis, split_axis=0, concat_axis=0, tiled=True)


def position_of(*axes):
    return jnp.stack([lax.axis_index(axis) for axis in axes]).astype(jnp.int32)


def pack_kernel(turn, gain, gate, up, down, out):
    copies, part, width = out.shape
    width = width // 3
    rows = gain.shape[1]
    row = lax.broadcasted_iota(jnp.int32, (part, rows), 0) + turn[0] * part
    column = lax.broadcasted_iota(jnp.int32, (part, rows), 1)
    factor = jnp.sum(jnp.where(row == column, gain[...], 0.0), axis=1, keepdims=True)
    for k, (source, scaled) in enumerate(((gate, True), (up, True), (down, False))):
        value = source[0]
        value = (factor * value if scaled else value).astype(jnp.bfloat16)
        for s in range(copies):
            out[s, :, k * width : (k + 1) * width] = value[:, s * width : (s + 1) * width]


def packed_weights(norm_gain, gate_weight, up_weight, down_weight, copies):
    experts, rows, columns = gate_weight.shape
    part = rows // lax.axis_size("grp")
    width = columns // copies
    block = pl.BlockSpec((1, part, columns), lambda e, turn: (e, turn[0], 0))
    return pl.pallas_call(
        pack_kernel,
        out_shape=jax.ShapeDtypeStruct((experts * copies, part, 3 * width), jnp.bfloat16),
        grid_spec=pltpu.PrefetchScalarGridSpec(
            num_scalar_prefetch=1,
            grid=(experts,),
            in_specs=[pl.BlockSpec((1, rows), lambda e, turn: (0, 0)), block, block, block],
            out_specs=pl.BlockSpec((copies, part, 3 * width), lambda e, turn: (e, 0, 0)),
        ),
        name="pack",
    )(position_of("grp"), norm_gain.reshape(1, rows), gate_weight, up_weight, down_weight)


def before_matrix(count):
    row = lax.broadcasted_iota(jnp.int32, (count, count), 0)
    column = lax.broadcasted_iota(jnp.int32, (count, count), 1)
    return jnp.where(row < column, 1.0, 0.0).astype(jnp.bfloat16)


def dispatch_kernel(routes, tokens, out):
    experts, capacity, _ = out.shape
    top, count = routes.shape
    expert = lax.broadcasted_iota(jnp.int32, (experts, count), 0)
    named = routes[0:1, :] == expert
    for k in range(1, top):
        named = named | (routes[k : k + 1, :] == expert)
    position = jnp.dot(
        jnp.where(named, 1.0, 0.0).astype(jnp.bfloat16),
        before_matrix(count),
        preferred_element_type=jnp.float32,
    )
    position = jnp.where(named, position.astype(jnp.int32), capacity)
    slot = lax.broadcasted_iota(jnp.int32, (capacity, count), 0)
    for e in range(experts):
        select = jnp.where(position[e : e + 1, :] == slot, 1.0, 0.0).astype(jnp.bfloat16)
        out[e] = jnp.dot(
            select, tokens[...], preferred_element_type=jnp.float32
        ).astype(jnp.bfloat16)


def dispatched(tokens, routes, experts, capacity):
    return pl.pallas_call(
        dispatch_kernel,
        out_shape=jax.ShapeDtypeStruct((experts, capacity, tokens.shape[1]), jnp.bfloat16),
        name="dispatch",
    )(routes.T, tokens)


def expert_kernel(span, count, groups, whole, place, *refs):
    first, share = span
    pieces, parts = refs[: 2 * groups], refs[2 * groups : 2 * groups + count]
    outs, assembled = refs[2 * groups + count : -2], refs[-2:]
    if whole:
        outs = [outs[0].at[k] for k in range(count)]
    copies, halves, _, cols = parts[0].shape
    part, width = pieces[0].shape[1], pieces[0].shape[2] // 3
    rows = copies * share
    for k in range(groups):
        index = lax.rem(place[3] + (groups - k), groups)
        for held, piece in zip(assembled, (pieces[k], pieces[groups + k])):
            held[:, pl.ds(index, 1)] = piece[...][:, None]

    def block(held, k, c, start, end, origin=place[0]):
        sources = cols // (groups * part)
        at = (lax.rem(origin + k, count) * halves + c) * sources
        return held[pl.ds(at, sources), :, :, start:end].reshape(cols, end - start)

    sums = [jnp.zeros((rows, 2 * width), jnp.float32) for _ in range(2)]
    squares = jnp.zeros((rows, cols), jnp.float32)
    for k in range(count):
        for c in range(halves):
            core = lax.rem(place[1] + (halves - c), halves)
            left = parts[k][:, c, first : first + share].reshape(rows, cols)
            wide = left.astype(jnp.float32)
            squares = squares + wide * wide
            sums = [
                value
                + jnp.dot(
                    left,
                    block(held, count - k, core, 0, 2 * width),
                    preferred_element_type=jnp.float32,
                )
                for value, held in zip(sums, assembled)
            ]
    features = count * halves * cols
    row_scale = lax.rsqrt(jnp.sum(squares, axis=1, keepdims=True) / features + epsilon)
    hidden = []
    for value in sums:
        value = value * row_scale
        gate, up = value[:, :width], value[:, width:]
        hidden.append((gate / (1.0 + jnp.exp(-gate)) * up).astype(jnp.bfloat16))
    hidden = jnp.concatenate(hidden, axis=1)
    for k, out in enumerate(outs):
        for c in range(halves):
            down = jnp.concatenate(
                [
                    block(held, k, c, 2 * width, 3 * width, 0 if whole else place[0])
                    for held in assembled
                ],
                axis=1,
            )
            value = lax.dot_general(
                hidden, down, (((1,), (1,)), ((), ())), preferred_element_type=jnp.float32
            ).astype(jnp.bfloat16)
            for r in range(copies):
                target = lax.rem(place[2] + (copies - r), copies)
                out[pl.ds(target, 1), c] = value[r * share : (r + 1) * share][None]


def whole_block(value):
    return pl.BlockSpec(value.shape, lambda t, place, rank=len(value.shape): (0,) * rank)


def expert_outputs(pieces, parts, span, whole):
    copies, halves, _, cols = parts[0].shape
    sources, part, triple = pieces[0].shape
    size = (copies, halves, span[1], cols)
    size = (len(parts), *size) if whole else size
    outs = [jax.ShapeDtypeStruct(size, jnp.bfloat16)] * (1 if whole else len(parts))
    inputs = (*pieces, *parts)
    held = pltpu.VMEM((sources, len(pieces) // 2, part, triple), jnp.bfloat16)
    return pl.pallas_call(
        functools.partial(expert_kernel, span, len(parts), len(pieces) // 2, whole),
        out_shape=outs,
        grid_spec=pltpu.PrefetchScalarGridSpec(
            num_scalar_prefetch=1,
            grid=(1,),
            in_specs=[whole_block(value) for value in inputs],
            out_specs=[whole_block(out) for out in outs],
            scratch_shapes=[held, held],
        ),
        compiler_params=vmem(32),
        name="experts",
    )(position_of("tp_x", "tp_c", "fs_lo", "grp"), *inputs)


def choose_kernel(routes, out):
    top, slots, count = out.shape
    capacity = count * 5 // 16
    expert = lax.broadcasted_iota(jnp.int32, (slots // capacity, count), 0)
    named = [routes[k : k + 1, :] == expert for k in range(top)]
    either = functools.reduce(jnp.logical_or, named)
    position = jnp.dot(
        jnp.where(either, 1.0, 0.0).astype(jnp.bfloat16),
        before_matrix(count),
        preferred_element_type=jnp.float32,
    ).astype(jnp.int32)
    slot = lax.broadcasted_iota(jnp.int32, (slots, count), 0)
    for k in range(top):
        mine = jnp.sum(
            jnp.where(named[k], expert * capacity + position, 0), axis=0, keepdims=True
        )
        out[k] = jnp.where(mine == slot, 1.0, 0.0).astype(jnp.bfloat16)


def chosen_slots(routes, slots):
    count, top = routes.shape
    return pl.pallas_call(
        choose_kernel,
        out_shape=jax.ShapeDtypeStruct((top, slots, count), jnp.bfloat16),
        compiler_params=vmem(12),
        name="choose",
    )(routes.T)


def combine_kernel(place, chosen, route_weights, returned, out):
    top, slots, _ = chosen.shape
    values = returned[...].reshape(slots, returned.shape[2])
    total = jnp.zeros(out.shape, jnp.float32)
    for k in range(top):
        picked = lax.dot_general(
            chosen[k], values, (((0,), (0,)), ((), ())), preferred_element_type=jnp.float32
        )
        total = total + route_weights[:, k : k + 1] * picked
    out[...] = total.astype(jnp.bfloat16)


def combined(chosen, route_weights, returned):
    out = jax.ShapeDtypeStruct((route_weights.shape[0], returned.shape[2]), jnp.bfloat16)
    inputs = (chosen, route_weights, returned)
    return pl.pallas_call(
        combine_kernel,
        out_shape=out,
        grid_spec=pltpu.PrefetchScalarGridSpec(
            num_scalar_prefetch=1,
            grid=(1,),
            in_specs=[whole_block(value) for value in inputs],
            out_specs=whole_block(out),
        ),
        compiler_params=vmem(12),
        name="combine",
    )(position_of("grp"), *inputs)


def assembled_weights(pieces, rows):
    groups = len(pieces)
    sources, part, triple = pieces[0].shape
    weights = jnp.zeros((sources, groups, part, triple), jnp.bfloat16)
    for k, piece in enumerate(pieces):
        weights = lax.dynamic_update_slice_in_dim(
            weights, piece[:, None], lax.rem(lax.axis_index("grp") + groups - k, groups), axis=1
        )
    return weights.reshape(sources * rows, triple)


def halved(blocks):
    copies, slots, cols = blocks.shape
    cores = lax.axis_size("tp_c")
    blocks = blocks.reshape(copies, cores, slots // cores, cols)
    halves = []
    for j in range(cores):
        half = lax.dynamic_index_in_dim(
            blocks, lax.rem(lax.axis_index("tp_c") + j, cores), axis=1, keepdims=False
        )
        halves.append(half if j == 0 else shifted(half, "tp_c", j))
    return jnp.stack(halves, axis=1)


def on_device(tokens, routes, route_weights, norm_gain, gate_weight, up_weight, down_weight):
    experts, rows, _ = gate_weight.shape
    copies = lax.axis_size("fs_lo")
    row_count, col_width = tokens.shape
    capacity = row_count * 5 // 16
    share = experts * capacity // lax.axis_size("tp_c")
    cut = share // 2
    spans = ((0, cut), (cut, share - cut))

    outgoing = dispatched(tokens, routes, experts, capacity)
    arrived = exchange(outgoing, "fs_hi")
    block = arrived.reshape(experts * capacity, col_width)
    blocks = [block] + [shifted(block, "fs_lo", k) for k in range(1, copies)]
    blocks = halved(jnp.stack(blocks))
    parts = [blocks] + [
        shifted(blocks, "tp_x", k) for k in range(1, lax.axis_size("tp_x"))
    ]

    packed = packed_weights(norm_gain, gate_weight, up_weight, down_weight, copies)
    mine = exchange(packed, FS)
    own = [mine] + [shifted(mine, "grp", k) for k in range(1, lax.axis_size("grp"))]
    other = [shifted(piece, "tp_c", 1) for piece in own]
    chosen = chosen_slots(routes, experts * capacity)

    sums = []
    for t, span in enumerate(spans):
        outs = expert_outputs(own + other, parts, span, t == 0)
        if t == 0:
            arrived = exchange(outs[0], "tp_x")
            got = [arrived[k] for k in range(len(parts))]
        else:
            got = [outs[0]] + [shifted(outs[k], "tp_x", k) for k in range(1, len(outs))]
        over_x = sum(value.astype(jnp.float32) for value in got).astype(jnp.bfloat16)
        sent = exchange(over_x.reshape(-1, *over_x.shape[2:]), ("fs_lo", "tp_c"))
        over_s = jnp.sum(sent.reshape(over_x.shape), axis=0, dtype=jnp.float32)
        sums.append(over_s.astype(jnp.bfloat16))
    own = assembled_weights(own, rows)
    back = jnp.concatenate(sums, axis=1).reshape(experts, capacity, col_width)
    returned = exchange(back, "fs_hi")
    width = own.shape[1] // 3
    outputs = [own[None, :, k * width : (k + 1) * width] for k in range(3)]
    return (*outputs, combined(chosen, route_weights, returned))


def solution(mesh):
    split = Mesh(
        mesh.devices.reshape(mesh.shape["grp"], mesh.shape["fs"] // 4, 4, 4, 2),
        ("grp", *FS, *TP),
    )
    rows = P(("grp", *FS), None)
    weight = P(None, FS, TP)
    taken = P(FS, "grp", TP)

    return jax.shard_map(
        on_device,
        mesh=split,
        in_specs=(P(("grp", *FS), TP), rows, rows, P(FS), weight, weight, weight),
        out_specs=(taken, taken, taken, P(("grp", *FS), TP)),
        check_vma=False,
    )
```

```python
import functools

import jax
import jax.numpy as jnp
from jax import lax
from jax.experimental import pallas as pl
from jax.experimental.pallas import tpu as pltpu
from jax.sharding import Mesh
from jax.sharding import PartitionSpec as P

FS = ("fs_hi", "fs_lo")
TP = ("tp_x", "tp_c")

epsilon = 1e-06


def shifted(value, axis, step):
    count = lax.axis_size(axis)
    return lax.ppermute(value, axis, [(k, (k + step) % count) for k in range(count)])


def vmem(mebibytes):
    return pltpu.CompilerParams(vmem_limit_bytes=mebibytes * 1024 * 1024)


def exchange(value, axis):
    return lax.all_to_all(value, axis, split_axis=0, concat_axis=0, tiled=True)


def position_of(*axes):
    return jnp.stack([lax.axis_index(axis) for axis in axes]).astype(jnp.int32)


def pack_kernel(turn, gain, gate, up, down, out):
    copies, part, width = out.shape
    width = width // 3
    rows = gain.shape[1]
    row = lax.broadcasted_iota(jnp.int32, (part, rows), 0) + turn[0] * part
    column = lax.broadcasted_iota(jnp.int32, (part, rows), 1)
    factor = jnp.sum(jnp.where(row == column, gain[...], 0.0), axis=1, keepdims=True)
    for k, (source, scaled) in enumerate(((gate, True), (up, True), (down, False))):
        value = source[0]
        value = (factor * value if scaled else value).astype(jnp.bfloat16)
        for s in range(copies):
            out[s, :, k * width : (k + 1) * width] = value[:, s * width : (s + 1) * width]


def packed_weights(norm_gain, gate_weight, up_weight, down_weight, copies):
    experts, rows, columns = gate_weight.shape
    part = rows // lax.axis_size("grp")
    width = columns // copies
    block = pl.BlockSpec((1, part, columns), lambda e, turn: (e, turn[0], 0))
    return pl.pallas_call(
        pack_kernel,
        out_shape=jax.ShapeDtypeStruct((experts * copies, part, 3 * width), jnp.bfloat16),
        grid_spec=pltpu.PrefetchScalarGridSpec(
            num_scalar_prefetch=1,
            grid=(experts,),
            in_specs=[pl.BlockSpec((1, rows), lambda e, turn: (0, 0)), block, block, block],
            out_specs=pl.BlockSpec((copies, part, 3 * width), lambda e, turn: (e, 0, 0)),
        ),
        name="pack",
    )(position_of("grp"), norm_gain.reshape(1, rows), gate_weight, up_weight, down_weight)


def before_matrix(count):
    row = lax.broadcasted_iota(jnp.int32, (count, count), 0)
    column = lax.broadcasted_iota(jnp.int32, (count, count), 1)
    return jnp.where(row < column, 1.0, 0.0).astype(jnp.bfloat16)


def dispatch_kernel(routes, tokens, out):
    experts, capacity, _ = out.shape
    top, count = routes.shape
    expert = lax.broadcasted_iota(jnp.int32, (experts, count), 0)
    named = routes[0:1, :] == expert
    for k in range(1, top):
        named = named | (routes[k : k + 1, :] == expert)
    position = jnp.dot(
        jnp.where(named, 1.0, 0.0).astype(jnp.bfloat16),
        before_matrix(count),
        preferred_element_type=jnp.float32,
    )
    position = jnp.where(named, position.astype(jnp.int32), capacity)
    slot = lax.broadcasted_iota(jnp.int32, (capacity, count), 0)
    for e in range(experts):
        select = jnp.where(position[e : e + 1, :] == slot, 1.0, 0.0).astype(jnp.bfloat16)
        out[e] = jnp.dot(
            select, tokens[...], preferred_element_type=jnp.float32
        ).astype(jnp.bfloat16)


def dispatched(tokens, routes, experts, capacity):
    return pl.pallas_call(
        dispatch_kernel,
        out_shape=jax.ShapeDtypeStruct((experts, capacity, tokens.shape[1]), jnp.bfloat16),
        name="dispatch",
    )(routes.T, tokens)


def hidden_kernel(bundles, place, *refs):
    parts, out, assembled = refs[2 * bundles : -3], refs[-3], refs[-2:]
    count, groups = len(parts), assembled[0].shape[1]
    copies, halves, tokens, cols = parts[0].shape
    part, width = assembled[0].shape[2], assembled[0].shape[3] // 2
    rows = copies * tokens
    for held, pieces in zip(assembled, (refs[:bundles], refs[bundles : 2 * bundles])):
        step = 0
        for piece in pieces:
            for k in range(piece.shape[0]):
                index = lax.rem(place[3] + (groups - step), groups)
                held[:, pl.ds(index, 1)] = piece[k, :, :, : 2 * width][:, None]
                step += 1

    def block(held, x, c):
        sources = cols // (groups * part)
        at = (lax.rem(x, count) * halves + c) * sources
        return held[pl.ds(at, sources)].reshape(cols, 2 * width)

    sums = [jnp.zeros((rows, 2 * width), jnp.float32) for _ in range(2)]
    squares = jnp.zeros((rows, cols), jnp.float32)
    for k in range(count):
        for c in range(halves):
            core = lax.rem(place[1] + (halves - c), halves)
            left = parts[k][:, c].reshape(rows, cols)
            wide = left.astype(jnp.float32)
            squares = squares + wide * wide
            sums = [
                value
                + jnp.dot(
                    left,
                    block(held, place[0] + (count - k), core),
                    preferred_element_type=jnp.float32,
                )
                for value, held in zip(sums, assembled)
            ]
    features = count * halves * cols
    row_scale = lax.rsqrt(jnp.sum(squares, axis=1, keepdims=True) / features + epsilon)
    for j, value in enumerate(sums):
        value = value * row_scale
        gate, up = value[:, :width], value[:, width:]
        hidden = (gate / (1.0 + jnp.exp(-gate)) * up).astype(jnp.bfloat16)
        out[:, :, j * width : (j + 1) * width] = hidden.reshape(copies, tokens, width)


def hidden_units(own, other, parts):
    copies, _, tokens, _ = parts[0].shape
    _, sources, part, triple = own[0].shape
    groups = sum(piece.shape[0] for piece in own)
    width = triple // 3
    out = jax.ShapeDtypeStruct((copies, tokens, 2 * width), jnp.bfloat16)
    inputs = (*own, *other, *parts)
    held = pltpu.VMEM((sources, groups, part, 2 * width), jnp.bfloat16)
    return pl.pallas_call(
        functools.partial(hidden_kernel, len(own)),
        out_shape=out,
        grid_spec=pltpu.PrefetchScalarGridSpec(
            num_scalar_prefetch=1,
            grid=(1,),
            in_specs=[whole_block(value) for value in inputs],
            out_specs=whole_block(out),
            scratch_shapes=[held, held],
        ),
        compiler_params=vmem(32),
        name="hidden",
    )(position_of("tp_x", "tp_c", "fs_lo", "grp"), *inputs)


def project_kernel(bundles, place, *refs):
    hidden, out, held = refs[2 * bundles : -2], refs[-2], refs[-1]
    count, groups = len(hidden), held.shape[2]
    copies, tokens, depth = hidden[0].shape
    halves, cols = out.shape[1], out.shape[3]
    width = depth // 2
    for j, pieces in enumerate((refs[:bundles], refs[bundles : 2 * bundles])):
        step = 0
        for piece in pieces:
            for k in range(piece.shape[1]):
                index = lax.rem(place[3] + (groups - step), groups)
                held[:, :, pl.ds(index, 1), :, j * width : (j + 1) * width] = piece[:, k][
                    :, :, None
                ]
                step += 1
    share = held.shape[1] // halves
    for c in range(halves):
        value = jnp.zeros((copies * tokens, cols), jnp.float32)
        for k in range(count):
            source = lax.rem(place[0] + (count - k), count)
            down = held[pl.ds(source, 1), c * share : (c + 1) * share].reshape(cols, depth)
            value = value + lax.dot_general(
                hidden[k][...].reshape(copies * tokens, depth),
                down,
                (((1,), (1,)), ((), ())),
                preferred_element_type=jnp.float32,
            )
        value = value.astype(jnp.bfloat16)
        for r in range(copies):
            target = lax.rem(place[2] + (copies - r), copies)
            out[pl.ds(target, 1), c] = value[r * tokens : (r + 1) * tokens][None]


def projected(own, other, hidden, halves):
    copies, tokens, depth = hidden[0].shape
    count, _, sources, part, _ = own[0].shape
    groups = sum(piece.shape[1] for piece in own)
    cols = sources * groups * part // halves
    out = jax.ShapeDtypeStruct((copies, halves, tokens, cols), jnp.bfloat16)
    inputs = (*own, *other, *hidden)
    return pl.pallas_call(
        functools.partial(project_kernel, len(own)),
        out_shape=out,
        grid_spec=pltpu.PrefetchScalarGridSpec(
            num_scalar_prefetch=1,
            grid=(1,),
            in_specs=[whole_block(value) for value in inputs],
            out_specs=whole_block(out),
            scratch_shapes=[pltpu.VMEM((count, sources, groups, part, depth), jnp.bfloat16)],
        ),
        compiler_params=vmem(32),
        name="project",
    )(position_of("tp_x", "tp_c", "fs_lo", "grp"), *inputs)


def whole_block(value):
    return pl.BlockSpec(value.shape, lambda t, place, rank=len(value.shape): (0,) * rank)


def choose_kernel(routes, out):
    top, slots, count = out.shape
    capacity = count * 5 // 16
    expert = lax.broadcasted_iota(jnp.int32, (slots // capacity, count), 0)
    named = [routes[k : k + 1, :] == expert for k in range(top)]
    either = functools.reduce(jnp.logical_or, named)
    position = jnp.dot(
        jnp.where(either, 1.0, 0.0).astype(jnp.bfloat16),
        before_matrix(count),
        preferred_element_type=jnp.float32,
    ).astype(jnp.int32)
    slot = lax.broadcasted_iota(jnp.int32, (slots, count), 0)
    for k in range(top):
        mine = jnp.sum(
            jnp.where(named[k], expert * capacity + position, 0), axis=0, keepdims=True
        )
        out[k] = jnp.where(mine == slot, 1.0, 0.0).astype(jnp.bfloat16)


def chosen_slots(routes, slots):
    count, top = routes.shape
    return pl.pallas_call(
        choose_kernel,
        out_shape=jax.ShapeDtypeStruct((top, slots, count), jnp.bfloat16),
        compiler_params=vmem(12),
        name="choose",
    )(routes.T)


def combine_kernel(place, chosen, route_weights, returned, out):
    top, slots, _ = chosen.shape
    values = returned[...].reshape(slots, returned.shape[2])
    total = jnp.zeros(out.shape, jnp.float32)
    for k in range(top):
        picked = lax.dot_general(
            chosen[k], values, (((0,), (0,)), ((), ())), preferred_element_type=jnp.float32
        )
        total = total + route_weights[:, k : k + 1] * picked
    out[...] = total.astype(jnp.bfloat16)


def combined(chosen, route_weights, returned):
    out = jax.ShapeDtypeStruct((route_weights.shape[0], returned.shape[2]), jnp.bfloat16)
    inputs = (chosen, route_weights, returned)
    return pl.pallas_call(
        combine_kernel,
        out_shape=out,
        grid_spec=pltpu.PrefetchScalarGridSpec(
            num_scalar_prefetch=1,
            grid=(1,),
            in_specs=[whole_block(value) for value in inputs],
            out_specs=whole_block(out),
        ),
        compiler_params=vmem(12),
        name="combine",
    )(position_of("grp"), *inputs)


def assembled_weights(pieces, rows):
    groups = len(pieces)
    sources, part, triple = pieces[0].shape
    weights = jnp.zeros((sources, groups, part, triple), jnp.bfloat16)
    for k, piece in enumerate(pieces):
        weights = lax.dynamic_update_slice_in_dim(
            weights, piece[:, None], lax.rem(lax.axis_index("grp") + groups - k, groups), axis=1
        )
    return weights.reshape(sources * rows, triple)


def halved(blocks):
    copies, slots, cols = blocks.shape
    cores = lax.axis_size("tp_c")
    blocks = blocks.reshape(copies, cores, slots // cores, cols)
    halves = []
    for j in range(cores):
        half = lax.dynamic_index_in_dim(
            blocks, lax.rem(lax.axis_index("tp_c") + j, cores), axis=1, keepdims=False
        )
        halves.append(half if j == 0 else shifted(half, "tp_c", j))
    return jnp.stack(halves, axis=1)


def on_device(tokens, routes, route_weights, norm_gain, gate_weight, up_weight, down_weight):
    experts, rows, _ = gate_weight.shape
    copies = lax.axis_size("fs_lo")
    row_count, col_width = tokens.shape
    capacity = row_count * 5 // 16

    outgoing = dispatched(tokens, routes, experts, capacity)
    arrived = exchange(outgoing, "fs_hi")
    block = arrived.reshape(experts * capacity, col_width)
    blocks = [block] + [shifted(block, "fs_lo", k) for k in range(1, copies)]
    blocks = halved(jnp.stack(blocks))
    parts = [blocks] + [
        shifted(blocks, "tp_x", k) for k in range(1, lax.axis_size("tp_x"))
    ]

    packed = packed_weights(norm_gain, gate_weight, up_weight, down_weight, copies)
    mine = exchange(packed, FS)
    passed = [shifted(mine, "grp", k) for k in range(1, lax.axis_size("grp"))]
    own = [mine[None]] + ([jnp.stack(passed)] if passed else [])
    other = []
    for piece in own:
        other.append(shifted(piece, "tp_c", 1))
    chosen = chosen_slots(routes, experts * capacity)
    turned, paired = [], []
    for t, piece in enumerate(own):
        down = piece[..., 2 * piece.shape[3] // 3 :]
        down = down.reshape(down.shape[0], lax.axis_size("tp_x"), -1, *down.shape[2:])
        turned.append(exchange(jnp.swapaxes(down, 0, 1), "tp_x"))
        paired.append(shifted(turned[t], "tp_c", 1))

    units = hidden_units(own, other, parts)
    units = [units] + [shifted(units, "tp_x", k) for k in range(1, len(parts))]
    over_x = projected(turned, paired, units, lax.axis_size("tp_c"))
    sent = exchange(over_x.reshape(-1, *over_x.shape[2:]), ("fs_lo", "tp_c"))
    over_s = jnp.sum(sent.reshape(over_x.shape), axis=0, dtype=jnp.float32)
    back = over_s.astype(jnp.bfloat16).reshape(experts, capacity, col_width)
    returned = exchange(back, "fs_hi")
    own = assembled_weights([mine, *passed], rows)
    width = own.shape[1] // 3
    outputs = [own[None, :, k * width : (k + 1) * width] for k in range(3)]
    return (*outputs, combined(chosen, route_weights, returned))


def solution(mesh):
    split = Mesh(
        mesh.devices.reshape(mesh.shape["grp"], mesh.shape["fs"] // 4, 4, 4, 2),
        ("grp", *FS, *TP),
    )
    rows = P(("grp", *FS), None)
    weight = P(None, FS, TP)
    taken = P(FS, "grp", TP)

    return jax.shard_map(
        on_device,
        mesh=split,
        in_specs=(P(("grp", *FS), TP), rows, rows, P(FS), weight, weight, weight),
        out_specs=(taken, taken, taken, P(("grp", *FS), TP)),
        check_vma=False,
    )
```

```python
import functools

import jax
import jax.numpy as jnp
from jax import lax
from jax.experimental import pallas as pl
from jax.experimental.pallas import tpu as pltpu
from jax.sharding import Mesh
from jax.sharding import PartitionSpec as P

FS = ("fs_hi", "fs_lo")
TP = ("tp_x", "tp_c")

epsilon = 1e-06


def shifted(value, axis, step):
    count = lax.axis_size(axis)
    return lax.ppermute(value, axis, [(k, (k + step) % count) for k in range(count)])


def vmem(mebibytes):
    return pltpu.CompilerParams(vmem_limit_bytes=mebibytes * 1024 * 1024)


def exchange(value, axis):
    return lax.all_to_all(value, axis, split_axis=0, concat_axis=0, tiled=True)


def position_of(*axes):
    return jnp.stack([lax.axis_index(axis) for axis in axes]).astype(jnp.int32)


def pack_kernel(turn, gain, gate, up, down, out):
    copies, part, width = out.shape
    width = width // 3
    rows = gain.shape[1]
    row = lax.broadcasted_iota(jnp.int32, (part, rows), 0) + turn[0] * part
    column = lax.broadcasted_iota(jnp.int32, (part, rows), 1)
    factor = jnp.sum(jnp.where(row == column, gain[...], 0.0), axis=1, keepdims=True)
    for k, (source, scaled) in enumerate(((gate, True), (up, True), (down, False))):
        value = source[0]
        value = (factor * value if scaled else value).astype(jnp.bfloat16)
        for s in range(copies):
            out[s, :, k * width : (k + 1) * width] = value[:, s * width : (s + 1) * width]


def packed_weights(norm_gain, gate_weight, up_weight, down_weight, copies):
    experts, rows, columns = gate_weight.shape
    part = rows // lax.axis_size("grp")
    width = columns // copies
    block = pl.BlockSpec((1, part, columns), lambda e, turn: (e, turn[0], 0))
    return pl.pallas_call(
        pack_kernel,
        out_shape=jax.ShapeDtypeStruct((experts * copies, part, 3 * width), jnp.bfloat16),
        grid_spec=pltpu.PrefetchScalarGridSpec(
            num_scalar_prefetch=1,
            grid=(experts,),
            in_specs=[pl.BlockSpec((1, rows), lambda e, turn: (0, 0)), block, block, block],
            out_specs=pl.BlockSpec((copies, part, 3 * width), lambda e, turn: (e, 0, 0)),
        ),
        name="pack",
    )(position_of("grp"), norm_gain.reshape(1, rows), gate_weight, up_weight, down_weight)


def before_matrix(count):
    row = lax.broadcasted_iota(jnp.int32, (count, count), 0)
    column = lax.broadcasted_iota(jnp.int32, (count, count), 1)
    return jnp.where(row < column, 1.0, 0.0).astype(jnp.bfloat16)


def dispatch_kernel(routes, tokens, out):
    experts, capacity, _ = out.shape
    top, count = routes.shape
    expert = lax.broadcasted_iota(jnp.int32, (experts, count), 0)
    named = routes[0:1, :] == expert
    for k in range(1, top):
        named = named | (routes[k : k + 1, :] == expert)
    position = jnp.dot(
        jnp.where(named, 1.0, 0.0).astype(jnp.bfloat16),
        before_matrix(count),
        preferred_element_type=jnp.float32,
    )
    position = jnp.where(named, position.astype(jnp.int32), capacity)
    slot = lax.broadcasted_iota(jnp.int32, (capacity, count), 0)
    for e in range(experts):
        select = jnp.where(position[e : e + 1, :] == slot, 1.0, 0.0).astype(jnp.bfloat16)
        out[e] = jnp.dot(
            select, tokens[...], preferred_element_type=jnp.float32
        ).astype(jnp.bfloat16)


def dispatched(tokens, routes, experts, capacity):
    return pl.pallas_call(
        dispatch_kernel,
        out_shape=jax.ShapeDtypeStruct((experts, capacity, tokens.shape[1]), jnp.bfloat16),
        name="dispatch",
    )(routes.T, tokens)


def hidden_kernel(bundles, place, *refs):
    parts, out, assembled = refs[2 * bundles : -3], refs[-3], refs[-2:]
    count, groups = len(parts), assembled[0].shape[1]
    copies, halves, tokens, cols = parts[0].shape
    part, width = assembled[0].shape[2], assembled[0].shape[3] // 2
    rows = copies * tokens
    for held, pieces in zip(assembled, (refs[:bundles], refs[bundles : 2 * bundles])):
        step = 0
        for piece in pieces:
            for k in range(piece.shape[0]):
                index = lax.rem(place[3] + (groups - step), groups)
                held[:, pl.ds(index, 1)] = piece[k][:, None]
                step += 1

    def block(held, x, c):
        sources = cols // (groups * part)
        at = (lax.rem(x, count) * halves + c) * sources
        return held[pl.ds(at, sources)].reshape(cols, 2 * width)

    sums = [jnp.zeros((rows, 2 * width), jnp.float32) for _ in range(2)]
    squares = jnp.zeros((rows, cols), jnp.float32)
    for k in range(count):
        for c in range(halves):
            core = lax.rem(place[1] + (halves - c), halves)
            left = parts[k][:, c].reshape(rows, cols)
            wide = left.astype(jnp.float32)
            squares = squares + wide * wide
            sums = [
                value
                + jnp.dot(
                    left,
                    block(held, place[0] + (count - k), core),
                    preferred_element_type=jnp.float32,
                )
                for value, held in zip(sums, assembled)
            ]
    features = count * halves * cols
    row_scale = lax.rsqrt(jnp.sum(squares, axis=1, keepdims=True) / features + epsilon)
    for j, value in enumerate(sums):
        value = value * row_scale
        gate, up = value[:, :width], value[:, width:]
        hidden = (gate / (1.0 + jnp.exp(-gate)) * up).astype(jnp.bfloat16)
        out[:, :, j * width : (j + 1) * width] = hidden.reshape(copies, tokens, width)


def hidden_units(own, other, parts):
    copies, _, tokens, _ = parts[0].shape
    _, sources, part, double = own[0].shape
    groups = sum(piece.shape[0] for piece in own)
    width = double // 2
    out = jax.ShapeDtypeStruct((copies, tokens, 2 * width), jnp.bfloat16)
    inputs = (*own, *other, *parts)
    held = pltpu.VMEM((sources, groups, part, 2 * width), jnp.bfloat16)
    return pl.pallas_call(
        functools.partial(hidden_kernel, len(own)),
        out_shape=out,
        grid_spec=pltpu.PrefetchScalarGridSpec(
            num_scalar_prefetch=1,
            grid=(1,),
            in_specs=[whole_block(value) for value in inputs],
            out_specs=whole_block(out),
            scratch_shapes=[held, held],
        ),
        compiler_params=vmem(32),
        name="hidden",
    )(position_of("tp_x", "tp_c", "fs_lo", "grp"), *inputs)


def project_kernel(bundles, place, *refs):
    hidden, out, held = refs[2 * bundles : -2], refs[-2], refs[-1]
    count, groups = len(hidden), held.shape[2]
    copies, tokens, depth = hidden[0].shape
    halves, cols = out.shape[1], out.shape[3]
    width = depth // 2
    for j, pieces in enumerate((refs[:bundles], refs[bundles : 2 * bundles])):
        step = 0
        for piece in pieces:
            for k in range(piece.shape[0]):
                index = lax.rem(place[3] + (groups - step), groups)
                held[:, :, pl.ds(index, 1), :, j * width : (j + 1) * width] = piece[k][
                    :, :, None
                ]
                step += 1
    share = held.shape[1] // halves
    for c in range(halves):
        value = jnp.zeros((copies * tokens, cols), jnp.float32)
        for k in range(count):
            source = lax.rem(place[0] + (count - k), count)
            down = held[pl.ds(source, 1), c * share : (c + 1) * share].reshape(cols, depth)
            value = value + lax.dot_general(
                hidden[k][...].reshape(copies * tokens, depth),
                down,
                (((1,), (1,)), ((), ())),
                preferred_element_type=jnp.float32,
            )
        value = value.astype(jnp.bfloat16)
        for r in range(copies):
            target = lax.rem(place[2] + (copies - r), copies)
            out[pl.ds(target, 1), c] = value[r * tokens : (r + 1) * tokens][None]


def projected(own, other, hidden, halves):
    copies, tokens, depth = hidden[0].shape
    _, count, sources, part, _ = own[0].shape
    groups = sum(piece.shape[0] for piece in own)
    cols = sources * groups * part // halves
    out = jax.ShapeDtypeStruct((copies, halves, tokens, cols), jnp.bfloat16)
    inputs = (*own, *other, *hidden)
    return pl.pallas_call(
        functools.partial(project_kernel, len(own)),
        out_shape=out,
        grid_spec=pltpu.PrefetchScalarGridSpec(
            num_scalar_prefetch=1,
            grid=(1,),
            in_specs=[whole_block(value) for value in inputs],
            out_specs=whole_block(out),
            scratch_shapes=[pltpu.VMEM((count, sources, groups, part, depth), jnp.bfloat16)],
        ),
        compiler_params=vmem(32),
        name="project",
    )(position_of("tp_x", "tp_c", "fs_lo", "grp"), *inputs)


def whole_block(value):
    return pl.BlockSpec(value.shape, lambda t, place, rank=len(value.shape): (0,) * rank)


def choose_kernel(routes, out):
    top, slots, count = out.shape
    capacity = count * 5 // 16
    expert = lax.broadcasted_iota(jnp.int32, (slots // capacity, count), 0)
    named = [routes[k : k + 1, :] == expert for k in range(top)]
    either = functools.reduce(jnp.logical_or, named)
    position = jnp.dot(
        jnp.where(either, 1.0, 0.0).astype(jnp.bfloat16),
        before_matrix(count),
        preferred_element_type=jnp.float32,
    ).astype(jnp.int32)
    slot = lax.broadcasted_iota(jnp.int32, (slots, count), 0)
    for k in range(top):
        mine = jnp.sum(
            jnp.where(named[k], expert * capacity + position, 0), axis=0, keepdims=True
        )
        out[k] = jnp.where(mine == slot, 1.0, 0.0).astype(jnp.bfloat16)


def chosen_slots(routes, slots):
    count, top = routes.shape
    return pl.pallas_call(
        choose_kernel,
        out_shape=jax.ShapeDtypeStruct((top, slots, count), jnp.bfloat16),
        compiler_params=vmem(12),
        name="choose",
    )(routes.T)


def combine_kernel(place, chosen, route_weights, returned, out):
    top, slots, _ = chosen.shape
    values = returned[...].reshape(slots, returned.shape[2])
    total = jnp.zeros(out.shape, jnp.float32)
    for k in range(top):
        picked = lax.dot_general(
            chosen[k], values, (((0,), (0,)), ((), ())), preferred_element_type=jnp.float32
        )
        total = total + route_weights[:, k : k + 1] * picked
    out[...] = total.astype(jnp.bfloat16)


def combined(chosen, route_weights, returned):
    out = jax.ShapeDtypeStruct((route_weights.shape[0], returned.shape[2]), jnp.bfloat16)
    inputs = (chosen, route_weights, returned)
    return pl.pallas_call(
        combine_kernel,
        out_shape=out,
        grid_spec=pltpu.PrefetchScalarGridSpec(
            num_scalar_prefetch=1,
            grid=(1,),
            in_specs=[whole_block(value) for value in inputs],
            out_specs=whole_block(out),
        ),
        compiler_params=vmem(12),
        name="combine",
    )(position_of("grp"), *inputs)


def assembled_weights(pieces, rows):
    groups = len(pieces)
    sources, part, triple = pieces[0].shape
    weights = jnp.zeros((sources, groups, part, triple), jnp.bfloat16)
    for k, piece in enumerate(pieces):
        weights = lax.dynamic_update_slice_in_dim(
            weights, piece[:, None], lax.rem(lax.axis_index("grp") + groups - k, groups), axis=1
        )
    return weights.reshape(sources * rows, triple)


def passed_on(value):
    passed = [shifted(value, "grp", k) for k in range(1, lax.axis_size("grp"))]
    pieces = [value[None]] + ([jnp.stack(passed)] if passed else [])
    pairs = []
    for piece in pieces:
        pairs.append(shifted(piece, "tp_c", 1))
    return pieces, pairs


def halved(blocks):
    copies, slots, cols = blocks.shape
    cores = lax.axis_size("tp_c")
    blocks = blocks.reshape(copies, cores, slots // cores, cols)
    halves = []
    for j in range(cores):
        half = lax.dynamic_index_in_dim(
            blocks, lax.rem(lax.axis_index("tp_c") + j, cores), axis=1, keepdims=False
        )
        halves.append(half if j == 0 else shifted(half, "tp_c", j))
    return jnp.stack(halves, axis=1)


def on_device(tokens, routes, route_weights, norm_gain, gate_weight, up_weight, down_weight):
    experts, rows, _ = gate_weight.shape
    copies = lax.axis_size("fs_lo")
    row_count, col_width = tokens.shape
    capacity = row_count * 5 // 16

    outgoing = dispatched(tokens, routes, experts, capacity)
    arrived = exchange(outgoing, "fs_hi")
    block = arrived.reshape(experts * capacity, col_width)
    blocks = [block] + [shifted(block, "fs_lo", k) for k in range(1, copies)]
    blocks = halved(jnp.stack(blocks))
    parts = [blocks] + [
        shifted(blocks, "tp_x", k) for k in range(1, lax.axis_size("tp_x"))
    ]

    packed = packed_weights(norm_gain, gate_weight, up_weight, down_weight, copies)
    mine = exchange(packed, FS)
    cut = 2 * mine.shape[2] // 3
    scaled, down = mine[..., :cut], mine[..., cut:]
    turned = exchange(down.reshape(lax.axis_size("tp_x"), -1, *down.shape[1:]), "tp_x")
    scaled, scaled_pairs = passed_on(scaled)
    turned, turned_pairs = passed_on(turned)
    downs = [down] + [shifted(down, "grp", k) for k in range(1, lax.axis_size("grp"))]
    chosen = chosen_slots(routes, experts * capacity)

    units = hidden_units(scaled, scaled_pairs, parts)
    units = [units] + [shifted(units, "tp_x", k) for k in range(1, len(parts))]
    over_x = projected(turned, turned_pairs, units, lax.axis_size("tp_c"))
    sent = exchange(over_x.reshape(-1, *over_x.shape[2:]), ("fs_lo", "tp_c"))
    over_s = jnp.sum(sent.reshape(over_x.shape), axis=0, dtype=jnp.float32)
    back = over_s.astype(jnp.bfloat16).reshape(experts, capacity, col_width)
    returned = exchange(back, "fs_hi")
    double = assembled_weights([piece for group in scaled for piece in group], rows)
    width = double.shape[1] // 2
    outputs = [double[None, :, :width], double[None, :, width:]]
    outputs.append(assembled_weights(downs, rows)[None])
    return (*outputs, combined(chosen, route_weights, returned))


def solution(mesh):
    split = Mesh(
        mesh.devices.reshape(mesh.shape["grp"], mesh.shape["fs"] // 4, 4, 4, 2),
        ("grp", *FS, *TP),
    )
    rows = P(("grp", *FS), None)
    weight = P(None, FS, TP)
    taken = P(FS, "grp", TP)

    return jax.shard_map(
        on_device,
        mesh=split,
        in_specs=(P(("grp", *FS), TP), rows, rows, P(FS), weight, weight, weight),
        out_specs=(taken, taken, taken, P(("grp", *FS), TP)),
        check_vma=False,
    )
```

```python
import functools

import jax
import jax.numpy as jnp
from jax import lax
from jax.experimental import pallas as pl
from jax.experimental.pallas import tpu as pltpu
from jax.sharding import Mesh
from jax.sharding import PartitionSpec as P

FS = ("fs_hi", "fs_lo")
TP = ("tp_x", "tp_c")

epsilon = 1e-06


def shifted(value, axis, step):
    count = lax.axis_size(axis)
    return lax.ppermute(value, axis, [(k, (k + step) % count) for k in range(count)])


def vmem(mebibytes):
    return pltpu.CompilerParams(vmem_limit_bytes=mebibytes * 1024 * 1024)


def exchange(value, axis):
    return lax.all_to_all(value, axis, split_axis=0, concat_axis=0, tiled=True)


def position_of(*axes):
    return jnp.stack([lax.axis_index(axis) for axis in axes]).astype(jnp.int32)


def pack_kernel(turn, gain, gate, up, down, out):
    copies, part, width = out.shape
    width = width // 3
    rows = gain.shape[1]
    row = lax.broadcasted_iota(jnp.int32, (part, rows), 0) + turn[0] * part
    column = lax.broadcasted_iota(jnp.int32, (part, rows), 1)
    factor = jnp.sum(jnp.where(row == column, gain[...], 0.0), axis=1, keepdims=True)
    for k, (source, scaled) in enumerate(((gate, True), (up, True), (down, False))):
        value = source[0]
        value = (factor * value if scaled else value).astype(jnp.bfloat16)
        for s in range(copies):
            out[s, :, k * width : (k + 1) * width] = value[:, s * width : (s + 1) * width]


def packed_weights(norm_gain, gate_weight, up_weight, down_weight, copies):
    experts, rows, columns = gate_weight.shape
    part = rows // lax.axis_size("grp")
    width = columns // copies
    block = pl.BlockSpec((1, part, columns), lambda e, turn: (e, turn[0], 0))
    return pl.pallas_call(
        pack_kernel,
        out_shape=jax.ShapeDtypeStruct((experts * copies, part, 3 * width), jnp.bfloat16),
        grid_spec=pltpu.PrefetchScalarGridSpec(
            num_scalar_prefetch=1,
            grid=(experts,),
            in_specs=[pl.BlockSpec((1, rows), lambda e, turn: (0, 0)), block, block, block],
            out_specs=pl.BlockSpec((copies, part, 3 * width), lambda e, turn: (e, 0, 0)),
        ),
        name="pack",
    )(position_of("grp"), norm_gain.reshape(1, rows), gate_weight, up_weight, down_weight)


def before_matrix(count):
    row = lax.broadcasted_iota(jnp.int32, (count, count), 0)
    column = lax.broadcasted_iota(jnp.int32, (count, count), 1)
    return jnp.where(row < column, 1.0, 0.0).astype(jnp.bfloat16)


def dispatch_kernel(routes, tokens, out):
    experts, capacity, _ = out.shape
    top, count = routes.shape
    expert = lax.broadcasted_iota(jnp.int32, (experts, count), 0)
    named = routes[0:1, :] == expert
    for k in range(1, top):
        named = named | (routes[k : k + 1, :] == expert)
    position = jnp.dot(
        jnp.where(named, 1.0, 0.0).astype(jnp.bfloat16),
        before_matrix(count),
        preferred_element_type=jnp.float32,
    )
    position = jnp.where(named, position.astype(jnp.int32), capacity)
    slot = lax.broadcasted_iota(jnp.int32, (capacity, count), 0)
    for e in range(experts):
        select = jnp.where(position[e : e + 1, :] == slot, 1.0, 0.0).astype(jnp.bfloat16)
        out[e] = jnp.dot(
            select, tokens[...], preferred_element_type=jnp.float32
        ).astype(jnp.bfloat16)


def dispatched(tokens, routes, experts, capacity):
    return pl.pallas_call(
        dispatch_kernel,
        out_shape=jax.ShapeDtypeStruct((experts, capacity, tokens.shape[1]), jnp.bfloat16),
        name="dispatch",
    )(routes.T, tokens)


def hidden_kernel(bundles, place, *refs):
    parts, out, assembled = refs[2 * bundles : -3], refs[-3], refs[-2:]
    count, groups = len(parts), assembled[0].shape[1]
    copies, halves, tokens, cols = parts[0].shape
    part, width = assembled[0].shape[2], assembled[0].shape[3] // 2
    rows = copies * tokens
    for held, pieces in zip(assembled, (refs[:bundles], refs[bundles : 2 * bundles])):
        step = 0
        for piece in pieces:
            for k in range(piece.shape[0]):
                index = lax.rem(place[3] + (groups - step), groups)
                held[:, pl.ds(index, 1)] = piece[k][:, None]
                step += 1

    def block(held, x, c):
        sources = cols // (groups * part)
        at = (lax.rem(x, count) * halves + c) * sources
        return held[pl.ds(at, sources)].reshape(cols, 2 * width)

    sums = [jnp.zeros((rows, 2 * width), jnp.float32) for _ in range(2)]
    squares = jnp.zeros((rows, cols), jnp.float32)
    for k in range(count):
        for c in range(halves):
            core = lax.rem(place[1] + (halves - c), halves)
            left = parts[k][:, c].reshape(rows, cols)
            wide = left.astype(jnp.float32)
            squares = squares + wide * wide
            sums = [
                value
                + jnp.dot(
                    left,
                    block(held, place[0] + (count - k), core),
                    preferred_element_type=jnp.float32,
                )
                for value, held in zip(sums, assembled)
            ]
    features = count * halves * cols
    row_scale = lax.rsqrt(jnp.sum(squares, axis=1, keepdims=True) / features + epsilon)
    for j, value in enumerate(sums):
        value = value * row_scale
        gate, up = value[:, :width], value[:, width:]
        hidden = (gate / (1.0 + jnp.exp(-gate)) * up).astype(jnp.bfloat16)
        out[:, :, j * width : (j + 1) * width] = hidden.reshape(copies, tokens, width)


def hidden_units(own, other, parts):
    copies, _, tokens, _ = parts[0].shape
    _, sources, part, double = own[0].shape
    groups = sum(piece.shape[0] for piece in own)
    width = double // 2
    out = jax.ShapeDtypeStruct((copies, tokens, 2 * width), jnp.bfloat16)
    inputs = (*own, *other, *parts)
    held = pltpu.VMEM((sources, groups, part, 2 * width), jnp.bfloat16)
    return pl.pallas_call(
        functools.partial(hidden_kernel, len(own)),
        out_shape=out,
        grid_spec=pltpu.PrefetchScalarGridSpec(
            num_scalar_prefetch=1,
            grid=(1,),
            in_specs=[whole_block(value) for value in inputs],
            out_specs=whole_block(out),
            scratch_shapes=[held, held],
        ),
        compiler_params=vmem(32),
        name="hidden",
    )(position_of("tp_x", "tp_c", "fs_lo", "grp"), *inputs)


def project_kernel(bundles, place, *refs):
    hidden, out, held = refs[2 * bundles : -2], refs[-2], refs[-1]
    count, groups = len(hidden), held.shape[2]
    copies, tokens, depth = hidden[0].shape
    halves, cols = out.shape[1], out.shape[3]
    width = depth // 2
    for j, pieces in enumerate((refs[:bundles], refs[bundles : 2 * bundles])):
        step = 0
        for piece in pieces:
            for k in range(piece.shape[0]):
                index = lax.rem(place[3] + (groups - step), groups)
                held[:, :, pl.ds(index, 1), :, j * width : (j + 1) * width] = piece[k][
                    :, :, None
                ]
                step += 1
    share = held.shape[1] // halves
    for c in range(halves):
        value = jnp.zeros((copies * tokens, cols), jnp.float32)
        for k in range(count):
            source = lax.rem(place[0] + (count - k), count)
            down = held[pl.ds(source, 1), c * share : (c + 1) * share].reshape(cols, depth)
            value = value + lax.dot_general(
                hidden[k][...].reshape(copies * tokens, depth),
                down,
                (((1,), (1,)), ((), ())),
                preferred_element_type=jnp.float32,
            )
        value = value.astype(jnp.bfloat16)
        for r in range(copies):
            target = lax.rem(place[2] + (copies - r), copies)
            out[pl.ds(target, 1), c] = value[r * tokens : (r + 1) * tokens][None]


def projected(own, other, hidden, halves):
    copies, tokens, depth = hidden[0].shape
    _, count, sources, part, _ = own[0].shape
    groups = sum(piece.shape[0] for piece in own)
    cols = sources * groups * part // halves
    out = jax.ShapeDtypeStruct((copies, halves, tokens, cols), jnp.bfloat16)
    inputs = (*own, *other, *hidden)
    return pl.pallas_call(
        functools.partial(project_kernel, len(own)),
        out_shape=out,
        grid_spec=pltpu.PrefetchScalarGridSpec(
            num_scalar_prefetch=1,
            grid=(1,),
            in_specs=[whole_block(value) for value in inputs],
            out_specs=whole_block(out),
            scratch_shapes=[pltpu.VMEM((count, sources, groups, part, depth), jnp.bfloat16)],
        ),
        compiler_params=vmem(32),
        name="project",
    )(position_of("tp_x", "tp_c", "fs_lo", "grp"), *inputs)


def whole_block(value):
    return pl.BlockSpec(value.shape, lambda t, place, rank=len(value.shape): (0,) * rank)


def choose_kernel(routes, out):
    top, slots, count = out.shape
    capacity = count * 5 // 16
    expert = lax.broadcasted_iota(jnp.int32, (slots // capacity, count), 0)
    named = [routes[k : k + 1, :] == expert for k in range(top)]
    either = functools.reduce(jnp.logical_or, named)
    position = jnp.dot(
        jnp.where(either, 1.0, 0.0).astype(jnp.bfloat16),
        before_matrix(count),
        preferred_element_type=jnp.float32,
    ).astype(jnp.int32)
    slot = lax.broadcasted_iota(jnp.int32, (slots, count), 0)
    for k in range(top):
        mine = jnp.sum(
            jnp.where(named[k], expert * capacity + position, 0), axis=0, keepdims=True
        )
        out[k] = jnp.where(mine == slot, 1.0, 0.0).astype(jnp.bfloat16)


def chosen_slots(routes, slots):
    count, top = routes.shape
    return pl.pallas_call(
        choose_kernel,
        out_shape=jax.ShapeDtypeStruct((top, slots, count), jnp.bfloat16),
        compiler_params=vmem(12),
        name="choose",
    )(routes.T)


def combine_kernel(place, chosen, route_weights, returned, out):
    top, slots, _ = chosen.shape
    values = returned[...].reshape(slots, returned.shape[2])
    total = jnp.zeros(out.shape, jnp.float32)
    for k in range(top):
        picked = lax.dot_general(
            chosen[k], values, (((0,), (0,)), ((), ())), preferred_element_type=jnp.float32
        )
        total = total + route_weights[:, k : k + 1] * picked
    out[...] = total.astype(jnp.bfloat16)


def combined(chosen, route_weights, returned):
    out = jax.ShapeDtypeStruct((route_weights.shape[0], returned.shape[2]), jnp.bfloat16)
    inputs = (chosen, route_weights, returned)
    return pl.pallas_call(
        combine_kernel,
        out_shape=out,
        grid_spec=pltpu.PrefetchScalarGridSpec(
            num_scalar_prefetch=1,
            grid=(1,),
            in_specs=[whole_block(value) for value in inputs],
            out_specs=whole_block(out),
        ),
        compiler_params=vmem(12),
        name="combine",
    )(position_of("grp"), *inputs)


def assembled_weights(pieces, rows):
    groups = len(pieces)
    sources, part, triple = pieces[0].shape
    weights = jnp.zeros((sources, groups, part, triple), jnp.bfloat16)
    for k, piece in enumerate(pieces):
        weights = lax.dynamic_update_slice_in_dim(
            weights, piece[:, None], lax.rem(lax.axis_index("grp") + groups - k, groups), axis=1
        )
    return weights.reshape(sources * rows, triple)


def split_kernel(mine, scaled, down):
    cut = scaled.shape[2]
    scaled[...] = mine[:, :, :cut]
    down[...] = mine[:, :, cut:]


def split_weights(mine):
    sources, part, triple = mine.shape
    cut = 2 * triple // 3
    step = sources // 4

    def spec(width):
        return pl.BlockSpec((step, part, width), lambda t: (t, 0, 0))

    return pl.pallas_call(
        split_kernel,
        out_shape=[
            jax.ShapeDtypeStruct((sources, part, width), jnp.bfloat16)
            for width in (cut, triple - cut)
        ],
        grid=(4,),
        in_specs=[spec(triple)],
        out_specs=[spec(cut), spec(triple - cut)],
        compiler_params=vmem(8),
        name="split",
    )(mine)


def passed_on(value):
    passed = [shifted(value, "grp", k) for k in range(1, lax.axis_size("grp"))]
    pieces = [value[None]] + ([jnp.stack(passed)] if passed else [])
    pairs = []
    for piece in pieces:
        pairs.append(shifted(piece, "tp_c", 1))
    return pieces, pairs


def halved(blocks):
    copies, slots, cols = blocks.shape
    cores = lax.axis_size("tp_c")
    blocks = blocks.reshape(copies, cores, slots // cores, cols)
    halves = []
    for j in range(cores):
        half = lax.dynamic_index_in_dim(
            blocks, lax.rem(lax.axis_index("tp_c") + j, cores), axis=1, keepdims=False
        )
        halves.append(half if j == 0 else shifted(half, "tp_c", j))
    return jnp.stack(halves, axis=1)


def on_device(tokens, routes, route_weights, norm_gain, gate_weight, up_weight, down_weight):
    experts, rows, _ = gate_weight.shape
    copies = lax.axis_size("fs_lo")
    row_count, col_width = tokens.shape
    capacity = row_count * 5 // 16

    outgoing = dispatched(tokens, routes, experts, capacity)
    arrived = exchange(outgoing, "fs_hi")
    block = arrived.reshape(experts * capacity, col_width)
    blocks = [block] + [shifted(block, "fs_lo", k) for k in range(1, copies)]
    blocks = halved(jnp.stack(blocks))
    parts = [blocks] + [
        shifted(blocks, "tp_x", k) for k in range(1, lax.axis_size("tp_x"))
    ]

    packed = packed_weights(norm_gain, gate_weight, up_weight, down_weight, copies)
    mine = exchange(packed, FS)
    scaled, down = split_weights(mine)
    turned = exchange(down.reshape(lax.axis_size("tp_x"), -1, *down.shape[1:]), "tp_x")
    scaled, scaled_pairs = passed_on(scaled)
    turned, turned_pairs = passed_on(turned)
    downs = [down] + [shifted(down, "grp", k) for k in range(1, lax.axis_size("grp"))]
    chosen = chosen_slots(routes, experts * capacity)

    units = hidden_units(scaled, scaled_pairs, parts)
    units = [units] + [shifted(units, "tp_x", k) for k in range(1, len(parts))]
    over_x = projected(turned, turned_pairs, units, lax.axis_size("tp_c"))
    sent = exchange(over_x.reshape(-1, *over_x.shape[2:]), ("fs_lo", "tp_c"))
    over_s = jnp.sum(sent.reshape(over_x.shape), axis=0, dtype=jnp.float32)
    back = over_s.astype(jnp.bfloat16).reshape(experts, capacity, col_width)
    returned = exchange(back, "fs_hi")
    double = assembled_weights([piece for group in scaled for piece in group], rows)
    width = double.shape[1] // 2
    outputs = [double[None, :, :width], double[None, :, width:]]
    outputs.append(assembled_weights(downs, rows)[None])
    return (*outputs, combined(chosen, route_weights, returned))


def solution(mesh):
    split = Mesh(
        mesh.devices.reshape(mesh.shape["grp"], mesh.shape["fs"] // 4, 4, 4, 2),
        ("grp", *FS, *TP),
    )
    rows = P(("grp", *FS), None)
    weight = P(None, FS, TP)
    taken = P(FS, "grp", TP)

    return jax.shard_map(
        on_device,
        mesh=split,
        in_specs=(P(("grp", *FS), TP), rows, rows, P(FS), weight, weight, weight),
        out_specs=(taken, taken, taken, P(("grp", *FS), TP)),
        check_vma=False,
    )
```

```python
import functools

import jax
import jax.numpy as jnp
from jax import lax
from jax.experimental import pallas as pl
from jax.experimental.pallas import tpu as pltpu
from jax.sharding import Mesh
from jax.sharding import PartitionSpec as P

FS = ("fs_hi", "fs_lo")
TP = ("tp_x", "tp_c")

epsilon = 1e-06


def shifted(value, axis, step):
    count = lax.axis_size(axis)
    return lax.ppermute(value, axis, [(k, (k + step) % count) for k in range(count)])


def vmem(mebibytes):
    return pltpu.CompilerParams(vmem_limit_bytes=mebibytes * 1024 * 1024)


def exchange(value, axis):
    return lax.all_to_all(value, axis, split_axis=0, concat_axis=0, tiled=True)


def position_of(*axes):
    return jnp.stack([lax.axis_index(axis) for axis in axes]).astype(jnp.int32)


def pack_kernel(turn, gain, gate, up, down, out):
    copies, part, width = out.shape
    width = width // 3
    rows = gain.shape[1]
    row = lax.broadcasted_iota(jnp.int32, (part, rows), 0) + turn[0] * part
    column = lax.broadcasted_iota(jnp.int32, (part, rows), 1)
    factor = jnp.sum(jnp.where(row == column, gain[...], 0.0), axis=1, keepdims=True)
    for k, (source, scaled) in enumerate(((gate, True), (up, True), (down, False))):
        value = source[0]
        value = (factor * value if scaled else value).astype(jnp.bfloat16)
        for s in range(copies):
            out[s, :, k * width : (k + 1) * width] = value[:, s * width : (s + 1) * width]


def packed_weights(norm_gain, gate_weight, up_weight, down_weight, copies):
    experts, rows, columns = gate_weight.shape
    part = rows // lax.axis_size("grp")
    width = columns // copies
    block = pl.BlockSpec((1, part, columns), lambda e, turn: (e, turn[0], 0))
    return pl.pallas_call(
        pack_kernel,
        out_shape=jax.ShapeDtypeStruct((experts * copies, part, 3 * width), jnp.bfloat16),
        grid_spec=pltpu.PrefetchScalarGridSpec(
            num_scalar_prefetch=1,
            grid=(experts,),
            in_specs=[pl.BlockSpec((1, rows), lambda e, turn: (0, 0)), block, block, block],
            out_specs=pl.BlockSpec((copies, part, 3 * width), lambda e, turn: (e, 0, 0)),
        ),
        name="pack",
    )(position_of("grp"), norm_gain.reshape(1, rows), gate_weight, up_weight, down_weight)


def before_matrix(count):
    row = lax.broadcasted_iota(jnp.int32, (count, count), 0)
    column = lax.broadcasted_iota(jnp.int32, (count, count), 1)
    return jnp.where(row < column, 1.0, 0.0).astype(jnp.bfloat16)


def dispatch_kernel(place, routes, tokens, *outs):
    experts = len(outs)
    capacity = outs[0].shape[0]
    top, count = routes.shape
    expert = lax.broadcasted_iota(jnp.int32, (experts, count), 0)
    named = routes[0:1, :] == expert
    for k in range(1, top):
        named = named | (routes[k : k + 1, :] == expert)
    position = jnp.dot(
        jnp.where(named, 1.0, 0.0).astype(jnp.bfloat16),
        before_matrix(count),
        preferred_element_type=jnp.float32,
    )
    position = jnp.where(named, position.astype(jnp.int32), capacity)
    slot = lax.broadcasted_iota(jnp.int32, (capacity, count), 0)
    for k, out in enumerate(outs):
        target = lax.rem(place[0] + k, experts)
        mine = jnp.sum(jnp.where(expert == target, position, 0), axis=0, keepdims=True)
        select = jnp.where(mine == slot, 1.0, 0.0).astype(jnp.bfloat16)
        out[...] = jnp.dot(
            select, tokens[...], preferred_element_type=jnp.float32
        ).astype(jnp.bfloat16)


def dispatched(tokens, routes, experts, capacity):
    out = jax.ShapeDtypeStruct((capacity, tokens.shape[1]), jnp.bfloat16)
    inputs = (routes.T, tokens)
    return pl.pallas_call(
        dispatch_kernel,
        out_shape=[out] * experts,
        grid_spec=pltpu.PrefetchScalarGridSpec(
            num_scalar_prefetch=1,
            grid=(1,),
            in_specs=[whole_block(value) for value in inputs],
            out_specs=[whole_block(out)] * experts,
        ),
        name="dispatch",
    )(position_of("fs_hi"), *inputs)


def gather_kernel(place, *refs):
    pieces, out = refs[:-1], refs[-1]
    for k, piece in enumerate(pieces):
        source = lax.rem(place[0] + (len(pieces) - k), len(pieces))
        out[pl.ds(source, 1)] = piece[...][None]


def in_order(pieces):
    out = jax.ShapeDtypeStruct((len(pieces), *pieces[0].shape), jnp.bfloat16)
    return pl.pallas_call(
        gather_kernel,
        out_shape=out,
        grid_spec=pltpu.PrefetchScalarGridSpec(
            num_scalar_prefetch=1,
            grid=(1,),
            in_specs=[whole_block(piece) for piece in pieces],
            out_specs=whole_block(out),
        ),
        compiler_params=vmem(8),
        name="gather",
    )(position_of("fs_hi"), *pieces)


def hidden_kernel(bundles, place, *refs):
    parts, out, assembled = refs[2 * bundles : -3], refs[-3], refs[-2:]
    count, groups = len(parts), assembled[0].shape[1]
    copies, halves, tokens, cols = parts[0].shape
    part, width = assembled[0].shape[2], assembled[0].shape[3] // 2
    rows = copies * tokens
    for held, pieces in zip(assembled, (refs[:bundles], refs[bundles : 2 * bundles])):
        step = 0
        for piece in pieces:
            for k in range(piece.shape[0]):
                index = lax.rem(place[3] + (groups - step), groups)
                held[:, pl.ds(index, 1)] = piece[k][:, None]
                step += 1

    def block(held, x, c):
        sources = cols // (groups * part)
        at = (lax.rem(x, count) * halves + c) * sources
        return held[pl.ds(at, sources)].reshape(cols, 2 * width)

    sums = [jnp.zeros((rows, 2 * width), jnp.float32) for _ in range(2)]
    squares = jnp.zeros((rows, cols), jnp.float32)
    for k in range(count):
        for c in range(halves):
            core = lax.rem(place[1] + (halves - c), halves)
            left = parts[k][:, c].reshape(rows, cols)
            wide = left.astype(jnp.float32)
            squares = squares + wide * wide
            sums = [
                value
                + jnp.dot(
                    left,
                    block(held, place[0] + (count - k), core),
                    preferred_element_type=jnp.float32,
                )
                for value, held in zip(sums, assembled)
            ]
    features = count * halves * cols
    row_scale = lax.rsqrt(jnp.sum(squares, axis=1, keepdims=True) / features + epsilon)
    for j, value in enumerate(sums):
        value = value * row_scale
        gate, up = value[:, :width], value[:, width:]
        hidden = (gate / (1.0 + jnp.exp(-gate)) * up).astype(jnp.bfloat16)
        out[:, :, j * width : (j + 1) * width] = hidden.reshape(copies, tokens, width)


def hidden_units(own, other, parts):
    copies, _, tokens, _ = parts[0].shape
    _, sources, part, double = own[0].shape
    groups = sum(piece.shape[0] for piece in own)
    width = double // 2
    out = jax.ShapeDtypeStruct((copies, tokens, 2 * width), jnp.bfloat16)
    inputs = (*own, *other, *parts)
    held = pltpu.VMEM((sources, groups, part, 2 * width), jnp.bfloat16)
    return pl.pallas_call(
        functools.partial(hidden_kernel, len(own)),
        out_shape=out,
        grid_spec=pltpu.PrefetchScalarGridSpec(
            num_scalar_prefetch=1,
            grid=(1,),
            in_specs=[whole_block(value) for value in inputs],
            out_specs=whole_block(out),
            scratch_shapes=[held, held],
        ),
        compiler_params=vmem(32),
        name="hidden",
    )(position_of("tp_x", "tp_c", "fs_lo", "grp"), *inputs)


def project_kernel(bundles, place, *refs):
    hidden, out, held = refs[2 * bundles : -2], refs[-2], refs[-1]
    count, groups = len(hidden), held.shape[2]
    copies, tokens, depth = hidden[0].shape
    halves, cols = out.shape[1], out.shape[3]
    width = depth // 2
    for j, pieces in enumerate((refs[:bundles], refs[bundles : 2 * bundles])):
        step = 0
        for piece in pieces:
            for k in range(piece.shape[0]):
                index = lax.rem(place[3] + (groups - step), groups)
                held[:, :, pl.ds(index, 1), :, j * width : (j + 1) * width] = piece[k][
                    :, :, None
                ]
                step += 1
    share = held.shape[1] // halves
    for c in range(halves):
        value = jnp.zeros((copies * tokens, cols), jnp.float32)
        for k in range(count):
            source = lax.rem(place[0] + (count - k), count)
            down = held[pl.ds(source, 1), c * share : (c + 1) * share].reshape(cols, depth)
            value = value + lax.dot_general(
                hidden[k][...].reshape(copies * tokens, depth),
                down,
                (((1,), (1,)), ((), ())),
                preferred_element_type=jnp.float32,
            )
        value = value.astype(jnp.bfloat16)
        for r in range(copies):
            target = lax.rem(place[2] + (copies - r), copies)
            out[pl.ds(target, 1), c] = value[r * tokens : (r + 1) * tokens][None]


def projected(own, other, hidden, halves):
    copies, tokens, depth = hidden[0].shape
    _, count, sources, part, _ = own[0].shape
    groups = sum(piece.shape[0] for piece in own)
    cols = sources * groups * part // halves
    out = jax.ShapeDtypeStruct((copies, halves, tokens, cols), jnp.bfloat16)
    inputs = (*own, *other, *hidden)
    return pl.pallas_call(
        functools.partial(project_kernel, len(own)),
        out_shape=out,
        grid_spec=pltpu.PrefetchScalarGridSpec(
            num_scalar_prefetch=1,
            grid=(1,),
            in_specs=[whole_block(value) for value in inputs],
            out_specs=whole_block(out),
            scratch_shapes=[pltpu.VMEM((count, sources, groups, part, depth), jnp.bfloat16)],
        ),
        compiler_params=vmem(32),
        name="project",
    )(position_of("tp_x", "tp_c", "fs_lo", "grp"), *inputs)


def whole_block(value):
    return pl.BlockSpec(value.shape, lambda t, place, rank=len(value.shape): (0,) * rank)


def choose_kernel(routes, out):
    top, slots, count = out.shape
    capacity = count * 5 // 16
    expert = lax.broadcasted_iota(jnp.int32, (slots // capacity, count), 0)
    named = [routes[k : k + 1, :] == expert for k in range(top)]
    either = functools.reduce(jnp.logical_or, named)
    position = jnp.dot(
        jnp.where(either, 1.0, 0.0).astype(jnp.bfloat16),
        before_matrix(count),
        preferred_element_type=jnp.float32,
    ).astype(jnp.int32)
    slot = lax.broadcasted_iota(jnp.int32, (slots, count), 0)
    for k in range(top):
        mine = jnp.sum(
            jnp.where(named[k], expert * capacity + position, 0), axis=0, keepdims=True
        )
        out[k] = jnp.where(mine == slot, 1.0, 0.0).astype(jnp.bfloat16)


def chosen_slots(routes, slots):
    count, top = routes.shape
    return pl.pallas_call(
        choose_kernel,
        out_shape=jax.ShapeDtypeStruct((top, slots, count), jnp.bfloat16),
        compiler_params=vmem(12),
        name="choose",
    )(routes.T)


def combine_kernel(place, chosen, route_weights, returned, out):
    top, slots, _ = chosen.shape
    values = returned[...].reshape(slots, returned.shape[2])
    total = jnp.zeros(out.shape, jnp.float32)
    for k in range(top):
        picked = lax.dot_general(
            chosen[k], values, (((0,), (0,)), ((), ())), preferred_element_type=jnp.float32
        )
        total = total + route_weights[:, k : k + 1] * picked
    out[...] = total.astype(jnp.bfloat16)


def combined(chosen, route_weights, returned):
    out = jax.ShapeDtypeStruct((route_weights.shape[0], returned.shape[2]), jnp.bfloat16)
    inputs = (chosen, route_weights, returned)
    return pl.pallas_call(
        combine_kernel,
        out_shape=out,
        grid_spec=pltpu.PrefetchScalarGridSpec(
            num_scalar_prefetch=1,
            grid=(1,),
            in_specs=[whole_block(value) for value in inputs],
            out_specs=whole_block(out),
        ),
        compiler_params=vmem(12),
        name="combine",
    )(position_of("grp"), *inputs)


def assembled_weights(pieces, rows):
    groups = len(pieces)
    sources, part, triple = pieces[0].shape
    weights = jnp.zeros((sources, groups, part, triple), jnp.bfloat16)
    for k, piece in enumerate(pieces):
        weights = lax.dynamic_update_slice_in_dim(
            weights, piece[:, None], lax.rem(lax.axis_index("grp") + groups - k, groups), axis=1
        )
    return weights.reshape(sources * rows, triple)


def split_kernel(mine, scaled, down):
    cut = scaled.shape[2]
    scaled[...] = mine[:, :, :cut]
    down[...] = mine[:, :, cut:]


def split_weights(mine):
    sources, part, triple = mine.shape
    cut = 2 * triple // 3
    step = sources // 4

    def spec(width):
        return pl.BlockSpec((step, part, width), lambda t: (t, 0, 0))

    return pl.pallas_call(
        split_kernel,
        out_shape=[
            jax.ShapeDtypeStruct((sources, part, width), jnp.bfloat16)
            for width in (cut, triple - cut)
        ],
        grid=(4,),
        in_specs=[spec(triple)],
        out_specs=[spec(cut), spec(triple - cut)],
        compiler_params=vmem(8),
        name="split",
    )(mine)


def passed_on(value):
    passed = [shifted(value, "grp", k) for k in range(1, lax.axis_size("grp"))]
    pieces = [value[None]] + ([jnp.stack(passed)] if passed else [])
    pairs = []
    for piece in pieces:
        pairs.append(shifted(piece, "tp_c", 1))
    return pieces, pairs


def halved(blocks):
    copies, slots, cols = blocks.shape
    cores = lax.axis_size("tp_c")
    blocks = blocks.reshape(copies, cores, slots // cores, cols)
    halves = []
    for j in range(cores):
        half = lax.dynamic_index_in_dim(
            blocks, lax.rem(lax.axis_index("tp_c") + j, cores), axis=1, keepdims=False
        )
        halves.append(half if j == 0 else shifted(half, "tp_c", j))
    return jnp.stack(halves, axis=1)


def on_device(tokens, routes, route_weights, norm_gain, gate_weight, up_weight, down_weight):
    experts, rows, _ = gate_weight.shape
    copies = lax.axis_size("fs_lo")
    row_count, col_width = tokens.shape
    capacity = row_count * 5 // 16

    outgoing = dispatched(tokens, routes, experts, capacity)
    arrived = [outgoing[0]] + [
        shifted(outgoing[k], "fs_hi", k) for k in range(1, experts)
    ]
    arrived = in_order(arrived)
    block = arrived.reshape(experts * capacity, col_width)
    blocks = [block] + [shifted(block, "fs_lo", k) for k in range(1, copies)]
    blocks = halved(jnp.stack(blocks))
    parts = [blocks] + [
        shifted(blocks, "tp_x", k) for k in range(1, lax.axis_size("tp_x"))
    ]

    packed = packed_weights(norm_gain, gate_weight, up_weight, down_weight, copies)
    mine = exchange(packed, FS)
    scaled, down = split_weights(mine)
    turned = exchange(down.reshape(lax.axis_size("tp_x"), -1, *down.shape[1:]), "tp_x")
    scaled, scaled_pairs = passed_on(scaled)
    turned, turned_pairs = passed_on(turned)
    downs = [down] + [shifted(down, "grp", k) for k in range(1, lax.axis_size("grp"))]
    chosen = chosen_slots(routes, experts * capacity)

    units = hidden_units(scaled, scaled_pairs, parts)
    units = [units] + [shifted(units, "tp_x", k) for k in range(1, len(parts))]
    over_x = projected(turned, turned_pairs, units, lax.axis_size("tp_c"))
    sent = exchange(over_x.reshape(-1, *over_x.shape[2:]), ("fs_lo", "tp_c"))
    over_s = jnp.sum(sent.reshape(over_x.shape), axis=0, dtype=jnp.float32)
    back = over_s.astype(jnp.bfloat16).reshape(experts, capacity, col_width)
    returned = exchange(back, "fs_hi")
    double = assembled_weights([piece for group in scaled for piece in group], rows)
    width = double.shape[1] // 2
    outputs = [double[None, :, :width], double[None, :, width:]]
    outputs.append(assembled_weights(downs, rows)[None])
    return (*outputs, combined(chosen, route_weights, returned))


def solution(mesh):
    split = Mesh(
        mesh.devices.reshape(mesh.shape["grp"], mesh.shape["fs"] // 4, 4, 4, 2),
        ("grp", *FS, *TP),
    )
    rows = P(("grp", *FS), None)
    weight = P(None, FS, TP)
    taken = P(FS, "grp", TP)

    return jax.shard_map(
        on_device,
        mesh=split,
        in_specs=(P(("grp", *FS), TP), rows, rows, P(FS), weight, weight, weight),
        out_specs=(taken, taken, taken, P(("grp", *FS), TP)),
        check_vma=False,
    )
```

```python
import functools

import jax
import jax.numpy as jnp
from jax import lax
from jax.experimental import pallas as pl
from jax.experimental.pallas import tpu as pltpu
from jax.sharding import Mesh
from jax.sharding import PartitionSpec as P

FS = ("fs_hi", "fs_lo")
TP = ("tp_x", "tp_c")

epsilon = 1e-06


def shifted(value, axis, step):
    count = lax.axis_size(axis)
    return lax.ppermute(value, axis, [(k, (k + step) % count) for k in range(count)])


def vmem(mebibytes):
    return pltpu.CompilerParams(vmem_limit_bytes=mebibytes * 1024 * 1024)


def exchange(value, axis):
    return lax.all_to_all(value, axis, split_axis=0, concat_axis=0, tiled=True)


def position_of(*axes):
    return jnp.stack([lax.axis_index(axis) for axis in axes]).astype(jnp.int32)


def pack_kernel(turn, gain, gate, up, down, out):
    copies, part, width = out.shape
    width = width // 3
    rows = gain.shape[1]
    row = lax.broadcasted_iota(jnp.int32, (part, rows), 0) + turn[0] * part
    column = lax.broadcasted_iota(jnp.int32, (part, rows), 1)
    factor = jnp.sum(jnp.where(row == column, gain[...], 0.0), axis=1, keepdims=True)
    for k, (source, scaled) in enumerate(((gate, True), (up, True), (down, False))):
        value = source[0]
        value = (factor * value if scaled else value).astype(jnp.bfloat16)
        for s in range(copies):
            out[s, :, k * width : (k + 1) * width] = value[:, s * width : (s + 1) * width]


def packed_weights(norm_gain, gate_weight, up_weight, down_weight, copies):
    experts, rows, columns = gate_weight.shape
    part = rows // lax.axis_size("grp")
    width = columns // copies
    block = pl.BlockSpec((1, part, columns), lambda e, turn: (e, turn[0], 0))
    return pl.pallas_call(
        pack_kernel,
        out_shape=jax.ShapeDtypeStruct((experts * copies, part, 3 * width), jnp.bfloat16),
        grid_spec=pltpu.PrefetchScalarGridSpec(
            num_scalar_prefetch=1,
            grid=(experts,),
            in_specs=[pl.BlockSpec((1, rows), lambda e, turn: (0, 0)), block, block, block],
            out_specs=pl.BlockSpec((copies, part, 3 * width), lambda e, turn: (e, 0, 0)),
        ),
        name="pack",
    )(position_of("grp"), norm_gain.reshape(1, rows), gate_weight, up_weight, down_weight)


def before_matrix(count):
    row = lax.broadcasted_iota(jnp.int32, (count, count), 0)
    column = lax.broadcasted_iota(jnp.int32, (count, count), 1)
    return jnp.where(row < column, 1.0, 0.0).astype(jnp.bfloat16)


def dispatch_kernel(routes, tokens, out):
    experts, capacity, _ = out.shape
    top, count = routes.shape
    expert = lax.broadcasted_iota(jnp.int32, (experts, count), 0)
    named = routes[0:1, :] == expert
    for k in range(1, top):
        named = named | (routes[k : k + 1, :] == expert)
    position = jnp.dot(
        jnp.where(named, 1.0, 0.0).astype(jnp.bfloat16),
        before_matrix(count),
        preferred_element_type=jnp.float32,
    )
    position = jnp.where(named, position.astype(jnp.int32), capacity)
    slot = lax.broadcasted_iota(jnp.int32, (capacity, count), 0)
    for e in range(experts):
        select = jnp.where(position[e : e + 1, :] == slot, 1.0, 0.0).astype(jnp.bfloat16)
        out[e] = jnp.dot(
            select, tokens[...], preferred_element_type=jnp.float32
        ).astype(jnp.bfloat16)


def dispatched(tokens, routes, experts, capacity):
    return pl.pallas_call(
        dispatch_kernel,
        out_shape=jax.ShapeDtypeStruct((experts, capacity, tokens.shape[1]), jnp.bfloat16),
        name="dispatch",
    )(routes.T, tokens)


def hidden_kernel(bundles, place, *refs):
    parts, out, assembled = refs[2 * bundles : -3], refs[-3], refs[-2:]
    count, groups = len(parts), assembled[0].shape[1]
    copies, halves, tokens, cols = parts[0].shape
    part, width = assembled[0].shape[2], assembled[0].shape[3] // 2
    rows = copies * tokens
    for held, pieces in zip(assembled, (refs[:bundles], refs[bundles : 2 * bundles])):
        step = 0
        for piece in pieces:
            for k in range(piece.shape[0]):
                index = lax.rem(place[3] + (groups - step), groups)
                held[:, pl.ds(index, 1)] = piece[k][:, None]
                step += 1

    def block(held, x, c):
        sources = cols // (groups * part)
        at = (lax.rem(x, count) * halves + c) * sources
        return held[pl.ds(at, sources)].reshape(cols, 2 * width)

    sums = [jnp.zeros((rows, 2 * width), jnp.float32) for _ in range(2)]
    squares = jnp.zeros((rows, cols), jnp.float32)
    for k in range(count):
        for c in range(halves):
            core = lax.rem(place[1] + (halves - c), halves)
            left = parts[k][:, c].reshape(rows, cols)
            wide = left.astype(jnp.float32)
            squares = squares + wide * wide
            sums = [
                value
                + jnp.dot(
                    left,
                    block(held, place[0] + (count - k), core),
                    preferred_element_type=jnp.float32,
                )
                for value, held in zip(sums, assembled)
            ]
    features = count * halves * cols
    row_scale = lax.rsqrt(jnp.sum(squares, axis=1, keepdims=True) / features + epsilon)
    for j, value in enumerate(sums):
        value = value * row_scale
        gate, up = value[:, :width], value[:, width:]
        hidden = (gate / (1.0 + jnp.exp(-gate)) * up).astype(jnp.bfloat16)
        hidden = hidden.reshape(copies, tokens, width)
        for k in range(count):
            out[k, :, :, j * width : (j + 1) * width] = hidden


def hidden_units(own, other, parts):
    copies, _, tokens, _ = parts[0].shape
    _, sources, part, double = own[0].shape
    groups = sum(piece.shape[0] for piece in own)
    width = double // 2
    out = jax.ShapeDtypeStruct((len(parts), copies, tokens, 2 * width), jnp.bfloat16)
    inputs = (*own, *other, *parts)
    held = pltpu.VMEM((sources, groups, part, 2 * width), jnp.bfloat16)
    return pl.pallas_call(
        functools.partial(hidden_kernel, len(own)),
        out_shape=out,
        grid_spec=pltpu.PrefetchScalarGridSpec(
            num_scalar_prefetch=1,
            grid=(1,),
            in_specs=[whole_block(value) for value in inputs],
            out_specs=whole_block(out),
            scratch_shapes=[held, held],
        ),
        compiler_params=vmem(32),
        name="hidden",
    )(position_of("tp_x", "tp_c", "fs_lo", "grp"), *inputs)


def project_kernel(bundles, place, *refs):
    hidden, out, held = refs[-3:]
    groups = held.shape[2]
    count, copies, tokens, depth = hidden.shape
    halves, cols = out.shape[1], out.shape[3]
    width = depth // 2
    for j, pieces in enumerate((refs[:bundles], refs[bundles : 2 * bundles])):
        step = 0
        for piece in pieces:
            for k in range(piece.shape[0]):
                index = lax.rem(place[3] + (groups - step), groups)
                held[:, :, pl.ds(index, 1), :, j * width : (j + 1) * width] = piece[k][
                    :, :, None
                ]
                step += 1
    share = held.shape[1] // halves
    for c in range(halves):
        value = jnp.zeros((copies * tokens, cols), jnp.float32)
        for k in range(count):
            down = held[k, c * share : (c + 1) * share].reshape(cols, depth)
            value = value + lax.dot_general(
                hidden[k].reshape(copies * tokens, depth),
                down,
                (((1,), (1,)), ((), ())),
                preferred_element_type=jnp.float32,
            )
        value = value.astype(jnp.bfloat16)
        for r in range(copies):
            target = lax.rem(place[2] + (copies - r), copies)
            out[pl.ds(target, 1), c] = value[r * tokens : (r + 1) * tokens][None]


def projected(own, other, hidden, halves):
    _, copies, tokens, depth = hidden.shape
    _, count, sources, part, _ = own[0].shape
    groups = sum(piece.shape[0] for piece in own)
    cols = sources * groups * part // halves
    out = jax.ShapeDtypeStruct((copies, halves, tokens, cols), jnp.bfloat16)
    inputs = (*own, *other, hidden)
    return pl.pallas_call(
        functools.partial(project_kernel, len(own)),
        out_shape=out,
        grid_spec=pltpu.PrefetchScalarGridSpec(
            num_scalar_prefetch=1,
            grid=(1,),
            in_specs=[whole_block(value) for value in inputs],
            out_specs=whole_block(out),
            scratch_shapes=[pltpu.VMEM((count, sources, groups, part, depth), jnp.bfloat16)],
        ),
        compiler_params=vmem(32),
        name="project",
    )(position_of("tp_x", "tp_c", "fs_lo", "grp"), *inputs)


def whole_block(value):
    return pl.BlockSpec(value.shape, lambda t, place, rank=len(value.shape): (0,) * rank)


def choose_kernel(routes, out):
    top, slots, count = out.shape
    capacity = count * 5 // 16
    expert = lax.broadcasted_iota(jnp.int32, (slots // capacity, count), 0)
    named = [routes[k : k + 1, :] == expert for k in range(top)]
    either = functools.reduce(jnp.logical_or, named)
    position = jnp.dot(
        jnp.where(either, 1.0, 0.0).astype(jnp.bfloat16),
        before_matrix(count),
        preferred_element_type=jnp.float32,
    ).astype(jnp.int32)
    slot = lax.broadcasted_iota(jnp.int32, (slots, count), 0)
    for k in range(top):
        mine = jnp.sum(
            jnp.where(named[k], expert * capacity + position, 0), axis=0, keepdims=True
        )
        out[k] = jnp.where(mine == slot, 1.0, 0.0).astype(jnp.bfloat16)


def chosen_slots(routes, slots):
    count, top = routes.shape
    return pl.pallas_call(
        choose_kernel,
        out_shape=jax.ShapeDtypeStruct((top, slots, count), jnp.bfloat16),
        compiler_params=vmem(12),
        name="choose",
    )(routes.T)


def combine_kernel(place, chosen, route_weights, returned, out):
    top, slots, _ = chosen.shape
    values = returned[...].reshape(slots, returned.shape[2])
    total = jnp.zeros(out.shape, jnp.float32)
    for k in range(top):
        picked = lax.dot_general(
            chosen[k], values, (((0,), (0,)), ((), ())), preferred_element_type=jnp.float32
        )
        total = total + route_weights[:, k : k + 1] * picked
    out[...] = total.astype(jnp.bfloat16)


def combined(chosen, route_weights, returned):
    out = jax.ShapeDtypeStruct((route_weights.shape[0], returned.shape[2]), jnp.bfloat16)
    inputs = (chosen, route_weights, returned)
    return pl.pallas_call(
        combine_kernel,
        out_shape=out,
        grid_spec=pltpu.PrefetchScalarGridSpec(
            num_scalar_prefetch=1,
            grid=(1,),
            in_specs=[whole_block(value) for value in inputs],
            out_specs=whole_block(out),
        ),
        compiler_params=vmem(12),
        name="combine",
    )(position_of("grp"), *inputs)


def assembled_weights(pieces, rows):
    groups = len(pieces)
    sources, part, triple = pieces[0].shape
    weights = jnp.zeros((sources, groups, part, triple), jnp.bfloat16)
    for k, piece in enumerate(pieces):
        weights = lax.dynamic_update_slice_in_dim(
            weights, piece[:, None], lax.rem(lax.axis_index("grp") + groups - k, groups), axis=1
        )
    return weights.reshape(sources * rows, triple)


def split_kernel(mine, scaled, down):
    cut = scaled.shape[2]
    scaled[...] = mine[:, :, :cut]
    down[...] = mine[:, :, cut:]


def split_weights(mine):
    sources, part, triple = mine.shape
    cut = 2 * triple // 3
    step = sources // 4

    def spec(width):
        return pl.BlockSpec((step, part, width), lambda t: (t, 0, 0))

    return pl.pallas_call(
        split_kernel,
        out_shape=[
            jax.ShapeDtypeStruct((sources, part, width), jnp.bfloat16)
            for width in (cut, triple - cut)
        ],
        grid=(4,),
        in_specs=[spec(triple)],
        out_specs=[spec(cut), spec(triple - cut)],
        compiler_params=vmem(8),
        name="split",
    )(mine)


def passed_on(value):
    passed = [shifted(value, "grp", k) for k in range(1, lax.axis_size("grp"))]
    pieces = [value[None]] + ([jnp.stack(passed)] if passed else [])
    pairs = []
    for piece in pieces:
        pairs.append(shifted(piece, "tp_c", 1))
    return pieces, pairs


def halved(blocks):
    copies, slots, cols = blocks.shape
    cores = lax.axis_size("tp_c")
    blocks = blocks.reshape(copies, cores, slots // cores, cols)
    halves = []
    for j in range(cores):
        half = lax.dynamic_index_in_dim(
            blocks, lax.rem(lax.axis_index("tp_c") + j, cores), axis=1, keepdims=False
        )
        halves.append(half if j == 0 else shifted(half, "tp_c", j))
    return jnp.stack(halves, axis=1)


def on_device(tokens, routes, route_weights, norm_gain, gate_weight, up_weight, down_weight):
    experts, rows, _ = gate_weight.shape
    copies = lax.axis_size("fs_lo")
    row_count, col_width = tokens.shape
    capacity = row_count * 5 // 16

    outgoing = dispatched(tokens, routes, experts, capacity)
    arrived = exchange(outgoing, "fs_hi")
    block = arrived.reshape(experts * capacity, col_width)
    blocks = [block] + [shifted(block, "fs_lo", k) for k in range(1, copies)]
    blocks = halved(jnp.stack(blocks))
    parts = [blocks] + [
        shifted(blocks, "tp_x", k) for k in range(1, lax.axis_size("tp_x"))
    ]

    packed = packed_weights(norm_gain, gate_weight, up_weight, down_weight, copies)
    mine = exchange(packed, FS)
    scaled, down = split_weights(mine)
    turned = exchange(down.reshape(lax.axis_size("tp_x"), -1, *down.shape[1:]), "tp_x")
    scaled, scaled_pairs = passed_on(scaled)
    turned, turned_pairs = passed_on(turned)
    downs = [down] + [shifted(down, "grp", k) for k in range(1, lax.axis_size("grp"))]
    chosen = chosen_slots(routes, experts * capacity)

    units = hidden_units(scaled, scaled_pairs, parts)
    units = exchange(units, "tp_x")
    over_x = projected(turned, turned_pairs, units, lax.axis_size("tp_c"))
    sent = exchange(over_x.reshape(-1, *over_x.shape[2:]), ("fs_lo", "tp_c"))
    over_s = jnp.sum(sent.reshape(over_x.shape), axis=0, dtype=jnp.float32)
    back = over_s.astype(jnp.bfloat16).reshape(experts, capacity, col_width)
    returned = exchange(back, "fs_hi")
    double = assembled_weights([piece for group in scaled for piece in group], rows)
    width = double.shape[1] // 2
    outputs = [double[None, :, :width], double[None, :, width:]]
    outputs.append(assembled_weights(downs, rows)[None])
    return (*outputs, combined(chosen, route_weights, returned))


def solution(mesh):
    split = Mesh(
        mesh.devices.reshape(mesh.shape["grp"], mesh.shape["fs"] // 4, 4, 4, 2),
        ("grp", *FS, *TP),
    )
    rows = P(("grp", *FS), None)
    weight = P(None, FS, TP)
    taken = P(FS, "grp", TP)

    return jax.shard_map(
        on_device,
        mesh=split,
        in_specs=(P(("grp", *FS), TP), rows, rows, P(FS), weight, weight, weight),
        out_specs=(taken, taken, taken, P(("grp", *FS), TP)),
        check_vma=False,
    )
```

```python
import functools

import jax
import jax.numpy as jnp
from jax import lax
from jax.experimental import pallas as pl
from jax.experimental.pallas import tpu as pltpu
from jax.sharding import Mesh
from jax.sharding import PartitionSpec as P

FS = ("fs_hi", "fs_lo")
TP = ("tp_x", "tp_c")

epsilon = 1e-06


def shifted(value, axis, step):
    count = lax.axis_size(axis)
    return lax.ppermute(value, axis, [(k, (k + step) % count) for k in range(count)])


def vmem(mebibytes):
    return pltpu.CompilerParams(vmem_limit_bytes=mebibytes * 1024 * 1024)


def paired(value, axis, flip):
    count = lax.axis_size(axis)
    return lax.ppermute(value, axis, [(k, k ^ flip) for k in range(count)])


def exchange(value, axis):
    return lax.all_to_all(value, axis, split_axis=0, concat_axis=0, tiled=True)


def position_of(*axes):
    return jnp.stack([lax.axis_index(axis) for axis in axes]).astype(jnp.int32)


def pack_kernel(turn, gain, gate, up, down, out):
    copies, part, width = out.shape
    width = width // 3
    rows = gain.shape[1]
    row = lax.broadcasted_iota(jnp.int32, (part, rows), 0) + turn[0] * part
    column = lax.broadcasted_iota(jnp.int32, (part, rows), 1)
    factor = jnp.sum(jnp.where(row == column, gain[...], 0.0), axis=1, keepdims=True)
    for k, (source, scaled) in enumerate(((gate, True), (up, True), (down, False))):
        value = source[0]
        value = (factor * value if scaled else value).astype(jnp.bfloat16)
        for s in range(copies):
            out[s, :, k * width : (k + 1) * width] = value[:, s * width : (s + 1) * width]


def packed_weights(norm_gain, gate_weight, up_weight, down_weight, copies):
    experts, rows, columns = gate_weight.shape
    part = rows // lax.axis_size("grp")
    width = columns // copies
    block = pl.BlockSpec((1, part, columns), lambda e, turn: (e, turn[0], 0))
    return pl.pallas_call(
        pack_kernel,
        out_shape=jax.ShapeDtypeStruct((experts * copies, part, 3 * width), jnp.bfloat16),
        grid_spec=pltpu.PrefetchScalarGridSpec(
            num_scalar_prefetch=1,
            grid=(experts,),
            in_specs=[pl.BlockSpec((1, rows), lambda e, turn: (0, 0)), block, block, block],
            out_specs=pl.BlockSpec((copies, part, 3 * width), lambda e, turn: (e, 0, 0)),
        ),
        name="pack",
    )(position_of("grp"), norm_gain.reshape(1, rows), gate_weight, up_weight, down_weight)


def before_matrix(count):
    row = lax.broadcasted_iota(jnp.int32, (count, count), 0)
    column = lax.broadcasted_iota(jnp.int32, (count, count), 1)
    return jnp.where(row < column, 1.0, 0.0).astype(jnp.bfloat16)


def dispatch_kernel(routes, tokens, out):
    experts, capacity, _ = out.shape
    top, count = routes.shape
    expert = lax.broadcasted_iota(jnp.int32, (experts, count), 0)
    named = routes[0:1, :] == expert
    for k in range(1, top):
        named = named | (routes[k : k + 1, :] == expert)
    position = jnp.dot(
        jnp.where(named, 1.0, 0.0).astype(jnp.bfloat16),
        before_matrix(count),
        preferred_element_type=jnp.float32,
    )
    position = jnp.where(named, position.astype(jnp.int32), capacity)
    slot = lax.broadcasted_iota(jnp.int32, (capacity, count), 0)
    for e in range(experts):
        select = jnp.where(position[e : e + 1, :] == slot, 1.0, 0.0).astype(jnp.bfloat16)
        out[e] = jnp.dot(
            select, tokens[...], preferred_element_type=jnp.float32
        ).astype(jnp.bfloat16)


def dispatched(tokens, routes, experts, capacity):
    return pl.pallas_call(
        dispatch_kernel,
        out_shape=jax.ShapeDtypeStruct((experts, capacity, tokens.shape[1]), jnp.bfloat16),
        name="dispatch",
    )(routes.T, tokens)


def hidden_kernel(bundles, place, *refs):
    parts, out, assembled = refs[2 * bundles : -3], refs[-3], refs[-2:]
    count, groups = len(parts), assembled[0].shape[1]
    copies, halves, tokens, cols = parts[0].shape
    part, width = assembled[0].shape[2], assembled[0].shape[3] // 2
    rows = copies * tokens
    for held, pieces in zip(assembled, (refs[:bundles], refs[bundles : 2 * bundles])):
        step = 0
        for piece in pieces:
            for k in range(piece.shape[0]):
                index = lax.rem(place[3] + (groups - step), groups)
                held[:, pl.ds(index, 1)] = piece[k][:, None]
                step += 1

    def block(held, x, c):
        sources = cols // (groups * part)
        at = (lax.rem(x, count) * halves + c) * sources
        return held[pl.ds(at, sources)].reshape(cols, 2 * width)

    sums = [jnp.zeros((rows, 2 * width), jnp.float32) for _ in range(2)]
    squares = jnp.zeros((rows, cols), jnp.float32)
    for k in range(count):
        for c in range(halves):
            core = lax.rem(place[1] + (halves - c), halves)
            left = parts[k][:, c].reshape(rows, cols)
            wide = left.astype(jnp.float32)
            squares = squares + wide * wide
            sums = [
                value
                + jnp.dot(
                    left,
                    block(held, place[0] + (count - k), core),
                    preferred_element_type=jnp.float32,
                )
                for value, held in zip(sums, assembled)
            ]
    features = count * halves * cols
    row_scale = lax.rsqrt(jnp.sum(squares, axis=1, keepdims=True) / features + epsilon)
    for j, value in enumerate(sums):
        value = value * row_scale
        gate, up = value[:, :width], value[:, width:]
        hidden = (gate / (1.0 + jnp.exp(-gate)) * up).astype(jnp.bfloat16)
        hidden = hidden.reshape(copies, tokens, width)
        for k in range(count):
            out[k, :, :, j * width : (j + 1) * width] = hidden


def hidden_units(own, other, parts):
    copies, _, tokens, _ = parts[0].shape
    _, sources, part, double = own[0].shape
    groups = sum(piece.shape[0] for piece in own)
    width = double // 2
    out = jax.ShapeDtypeStruct((len(parts), copies, tokens, 2 * width), jnp.bfloat16)
    inputs = (*own, *other, *parts)
    held = pltpu.VMEM((sources, groups, part, 2 * width), jnp.bfloat16)
    return pl.pallas_call(
        functools.partial(hidden_kernel, len(own)),
        out_shape=out,
        grid_spec=pltpu.PrefetchScalarGridSpec(
            num_scalar_prefetch=1,
            grid=(1,),
            in_specs=[whole_block(value) for value in inputs],
            out_specs=whole_block(out),
            scratch_shapes=[held, held],
        ),
        compiler_params=vmem(32),
        name="hidden",
    )(position_of("tp_x", "tp_c", "fs_lo", "grp"), *inputs)


def project_kernel(bundles, place, *refs):
    hidden, out, held = refs[-3:]
    groups = held.shape[2]
    count, copies, tokens, depth = hidden.shape
    halves, cols = out.shape[1], out.shape[3]
    width = depth // 2
    for j, pieces in enumerate((refs[:bundles], refs[bundles : 2 * bundles])):
        step = 0
        for piece in pieces:
            for k in range(piece.shape[0]):
                index = lax.rem(place[3] + (groups - step), groups)
                held[:, :, pl.ds(index, 1), :, j * width : (j + 1) * width] = piece[k][
                    :, :, None
                ]
                step += 1
    share = held.shape[1] // halves
    for c in range(halves):
        value = jnp.zeros((copies * tokens, cols), jnp.float32)
        for k in range(count):
            down = held[k, c * share : (c + 1) * share].reshape(cols, depth)
            value = value + lax.dot_general(
                hidden[k].reshape(copies * tokens, depth),
                down,
                (((1,), (1,)), ((), ())),
                preferred_element_type=jnp.float32,
            )
        value = value.astype(jnp.bfloat16)
        for r in range(copies):
            target = place[2] ^ r
            out[pl.ds(target, 1), c] = value[r * tokens : (r + 1) * tokens][None]


def projected(own, other, hidden, halves):
    _, copies, tokens, depth = hidden.shape
    _, count, sources, part, _ = own[0].shape
    groups = sum(piece.shape[0] for piece in own)
    cols = sources * groups * part // halves
    out = jax.ShapeDtypeStruct((copies, halves, tokens, cols), jnp.bfloat16)
    inputs = (*own, *other, hidden)
    return pl.pallas_call(
        functools.partial(project_kernel, len(own)),
        out_shape=out,
        grid_spec=pltpu.PrefetchScalarGridSpec(
            num_scalar_prefetch=1,
            grid=(1,),
            in_specs=[whole_block(value) for value in inputs],
            out_specs=whole_block(out),
            scratch_shapes=[pltpu.VMEM((count, sources, groups, part, depth), jnp.bfloat16)],
        ),
        compiler_params=vmem(32),
        name="project",
    )(position_of("tp_x", "tp_c", "fs_lo", "grp"), *inputs)


def whole_block(value):
    return pl.BlockSpec(value.shape, lambda t, place, rank=len(value.shape): (0,) * rank)


def choose_kernel(routes, out):
    top, slots, count = out.shape
    capacity = count * 5 // 16
    expert = lax.broadcasted_iota(jnp.int32, (slots // capacity, count), 0)
    named = [routes[k : k + 1, :] == expert for k in range(top)]
    either = functools.reduce(jnp.logical_or, named)
    position = jnp.dot(
        jnp.where(either, 1.0, 0.0).astype(jnp.bfloat16),
        before_matrix(count),
        preferred_element_type=jnp.float32,
    ).astype(jnp.int32)
    slot = lax.broadcasted_iota(jnp.int32, (slots, count), 0)
    for k in range(top):
        mine = jnp.sum(
            jnp.where(named[k], expert * capacity + position, 0), axis=0, keepdims=True
        )
        out[k] = jnp.where(mine == slot, 1.0, 0.0).astype(jnp.bfloat16)


def chosen_slots(routes, slots):
    count, top = routes.shape
    return pl.pallas_call(
        choose_kernel,
        out_shape=jax.ShapeDtypeStruct((top, slots, count), jnp.bfloat16),
        compiler_params=vmem(12),
        name="choose",
    )(routes.T)


def combine_kernel(place, chosen, route_weights, returned, out):
    top, slots, _ = chosen.shape
    values = returned[...].reshape(slots, returned.shape[2])
    total = jnp.zeros(out.shape, jnp.float32)
    for k in range(top):
        picked = lax.dot_general(
            chosen[k], values, (((0,), (0,)), ((), ())), preferred_element_type=jnp.float32
        )
        total = total + route_weights[:, k : k + 1] * picked
    out[...] = total.astype(jnp.bfloat16)


def combined(chosen, route_weights, returned):
    out = jax.ShapeDtypeStruct((route_weights.shape[0], returned.shape[2]), jnp.bfloat16)
    inputs = (chosen, route_weights, returned)
    return pl.pallas_call(
        combine_kernel,
        out_shape=out,
        grid_spec=pltpu.PrefetchScalarGridSpec(
            num_scalar_prefetch=1,
            grid=(1,),
            in_specs=[whole_block(value) for value in inputs],
            out_specs=whole_block(out),
        ),
        compiler_params=vmem(12),
        name="combine",
    )(position_of("grp"), *inputs)


def assembled_weights(pieces, rows):
    groups = len(pieces)
    sources, part, triple = pieces[0].shape
    weights = jnp.zeros((sources, groups, part, triple), jnp.bfloat16)
    for k, piece in enumerate(pieces):
        weights = lax.dynamic_update_slice_in_dim(
            weights, piece[:, None], lax.rem(lax.axis_index("grp") + groups - k, groups), axis=1
        )
    return weights.reshape(sources * rows, triple)


def split_kernel(mine, scaled, down):
    cut = scaled.shape[2]
    scaled[...] = mine[:, :, :cut]
    down[...] = mine[:, :, cut:]


def split_weights(mine):
    sources, part, triple = mine.shape
    cut = 2 * triple // 3
    step = sources // 4

    def spec(width):
        return pl.BlockSpec((step, part, width), lambda t: (t, 0, 0))

    return pl.pallas_call(
        split_kernel,
        out_shape=[
            jax.ShapeDtypeStruct((sources, part, width), jnp.bfloat16)
            for width in (cut, triple - cut)
        ],
        grid=(4,),
        in_specs=[spec(triple)],
        out_specs=[spec(cut), spec(triple - cut)],
        compiler_params=vmem(8),
        name="split",
    )(mine)


def passed_on(value):
    passed = [shifted(value, "grp", k) for k in range(1, lax.axis_size("grp"))]
    pieces = [value[None]] + ([jnp.stack(passed)] if passed else [])
    pairs = []
    for piece in pieces:
        pairs.append(shifted(piece, "tp_c", 1))
    return pieces, pairs


def halved(blocks):
    copies, slots, cols = blocks.shape
    cores = lax.axis_size("tp_c")
    blocks = blocks.reshape(copies, cores, slots // cores, cols)
    halves = []
    for j in range(cores):
        half = lax.dynamic_index_in_dim(
            blocks, lax.rem(lax.axis_index("tp_c") + j, cores), axis=1, keepdims=False
        )
        halves.append(half if j == 0 else shifted(half, "tp_c", j))
    return jnp.stack(halves, axis=1)


def on_device(tokens, routes, route_weights, norm_gain, gate_weight, up_weight, down_weight):
    experts, rows, _ = gate_weight.shape
    copies = lax.axis_size("fs_lo")
    row_count, col_width = tokens.shape
    capacity = row_count * 5 // 16

    outgoing = dispatched(tokens, routes, experts, capacity)
    arrived = exchange(outgoing, "fs_hi")
    block = arrived.reshape(experts * capacity, col_width)
    blocks = [block] + [paired(block, "fs_lo", k) for k in range(1, copies)]
    blocks = halved(jnp.stack(blocks))
    parts = [blocks] + [
        shifted(blocks, "tp_x", k) for k in range(1, lax.axis_size("tp_x"))
    ]

    packed = packed_weights(norm_gain, gate_weight, up_weight, down_weight, copies)
    mine = exchange(packed, FS)
    scaled, down = split_weights(mine)
    turned = exchange(down.reshape(lax.axis_size("tp_x"), -1, *down.shape[1:]), "tp_x")
    scaled, scaled_pairs = passed_on(scaled)
    turned, turned_pairs = passed_on(turned)
    downs = [down] + [shifted(down, "grp", k) for k in range(1, lax.axis_size("grp"))]
    chosen = chosen_slots(routes, experts * capacity)

    units = hidden_units(scaled, scaled_pairs, parts)
    units = exchange(units, "tp_x")
    over_x = projected(turned, turned_pairs, units, lax.axis_size("tp_c"))
    sent = exchange(over_x.reshape(-1, *over_x.shape[2:]), ("fs_lo", "tp_c"))
    over_s = jnp.sum(sent.reshape(over_x.shape), axis=0, dtype=jnp.float32)
    back = over_s.astype(jnp.bfloat16).reshape(experts, capacity, col_width)
    returned = exchange(back, "fs_hi")
    double = assembled_weights([piece for group in scaled for piece in group], rows)
    width = double.shape[1] // 2
    outputs = [double[None, :, :width], double[None, :, width:]]
    outputs.append(assembled_weights(downs, rows)[None])
    return (*outputs, combined(chosen, route_weights, returned))


def solution(mesh):
    split = Mesh(
        mesh.devices.reshape(mesh.shape["grp"], mesh.shape["fs"] // 4, 4, 4, 2),
        ("grp", *FS, *TP),
    )
    rows = P(("grp", *FS), None)
    weight = P(None, FS, TP)
    taken = P(FS, "grp", TP)

    return jax.shard_map(
        on_device,
        mesh=split,
        in_specs=(P(("grp", *FS), TP), rows, rows, P(FS), weight, weight, weight),
        out_specs=(taken, taken, taken, P(("grp", *FS), TP)),
        check_vma=False,
    )
```

```python
import functools

import jax
import jax.numpy as jnp
from jax import lax
from jax.experimental import pallas as pl
from jax.experimental.pallas import tpu as pltpu
from jax.sharding import Mesh
from jax.sharding import PartitionSpec as P

FS = ("fs_hi", "fs_lo")
TP = ("tp_x", "tp_c")

epsilon = 1e-06


def shifted(value, axis, step):
    count = lax.axis_size(axis)
    return lax.ppermute(value, axis, [(k, (k + step) % count) for k in range(count)])


def vmem(mebibytes):
    return pltpu.CompilerParams(vmem_limit_bytes=mebibytes * 1024 * 1024)


def paired(value, axis, flip):
    count = lax.axis_size(axis)
    return lax.ppermute(value, axis, [(k, k ^ flip) for k in range(count)])


def exchange(value, axis):
    return lax.all_to_all(value, axis, split_axis=0, concat_axis=0, tiled=True)


def position_of(*axes):
    return jnp.stack([lax.axis_index(axis) for axis in axes]).astype(jnp.int32)


def pack_kernel(turn, gain, gate, up, down, out):
    copies, part, width = out.shape
    width = width // 3
    rows = gain.shape[1]
    row = lax.broadcasted_iota(jnp.int32, (part, rows), 0) + turn[0] * part
    column = lax.broadcasted_iota(jnp.int32, (part, rows), 1)
    factor = jnp.sum(jnp.where(row == column, gain[...], 0.0), axis=1, keepdims=True)
    for k, (source, scaled) in enumerate(((gate, True), (up, True), (down, False))):
        value = source[0]
        value = (factor * value if scaled else value).astype(jnp.bfloat16)
        for s in range(copies):
            out[s, :, k * width : (k + 1) * width] = value[:, s * width : (s + 1) * width]


def packed_weights(norm_gain, gate_weight, up_weight, down_weight, copies):
    experts, rows, columns = gate_weight.shape
    part = rows // lax.axis_size("grp")
    width = columns // copies
    block = pl.BlockSpec((1, part, columns), lambda e, turn: (e, turn[0], 0))
    return pl.pallas_call(
        pack_kernel,
        out_shape=jax.ShapeDtypeStruct((experts * copies, part, 3 * width), jnp.bfloat16),
        grid_spec=pltpu.PrefetchScalarGridSpec(
            num_scalar_prefetch=1,
            grid=(experts,),
            in_specs=[pl.BlockSpec((1, rows), lambda e, turn: (0, 0)), block, block, block],
            out_specs=pl.BlockSpec((copies, part, 3 * width), lambda e, turn: (e, 0, 0)),
        ),
        name="pack",
    )(position_of("grp"), norm_gain.reshape(1, rows), gate_weight, up_weight, down_weight)


def before_matrix(count):
    row = lax.broadcasted_iota(jnp.int32, (count, count), 0)
    column = lax.broadcasted_iota(jnp.int32, (count, count), 1)
    return jnp.where(row < column, 1.0, 0.0).astype(jnp.bfloat16)


def dispatch_kernel(routes, tokens, out):
    experts, capacity, _ = out.shape
    top, count = routes.shape
    expert = lax.broadcasted_iota(jnp.int32, (experts, count), 0)
    named = routes[0:1, :] == expert
    for k in range(1, top):
        named = named | (routes[k : k + 1, :] == expert)
    position = jnp.dot(
        jnp.where(named, 1.0, 0.0).astype(jnp.bfloat16),
        before_matrix(count),
        preferred_element_type=jnp.float32,
    )
    position = jnp.where(named, position.astype(jnp.int32), capacity)
    slot = lax.broadcasted_iota(jnp.int32, (capacity, count), 0)
    select = jnp.concatenate(
        [jnp.where(position[e : e + 1, :] == slot, 1.0, 0.0) for e in range(experts)], axis=0
    ).astype(jnp.bfloat16)
    packed = jnp.dot(select, tokens[...], preferred_element_type=jnp.float32)
    for e in range(experts):
        out[e] = packed[e * capacity : (e + 1) * capacity].astype(jnp.bfloat16)


def dispatched(tokens, routes, experts, capacity):
    return pl.pallas_call(
        dispatch_kernel,
        out_shape=jax.ShapeDtypeStruct((experts, capacity, tokens.shape[1]), jnp.bfloat16),
        name="dispatch",
    )(routes.T, tokens)


def hidden_kernel(bundles, place, *refs):
    parts, out, assembled = refs[2 * bundles : -3], refs[-3], refs[-2:]
    count, groups = len(parts), assembled[0].shape[1]
    copies, halves, tokens, cols = parts[0].shape
    part, width = assembled[0].shape[2], assembled[0].shape[3] // 2
    rows = copies * tokens
    for held, pieces in zip(assembled, (refs[:bundles], refs[bundles : 2 * bundles])):
        step = 0
        for piece in pieces:
            for k in range(piece.shape[0]):
                index = lax.rem(place[3] + (groups - step), groups)
                held[:, pl.ds(index, 1)] = piece[k][:, None]
                step += 1

    def block(held, x, c):
        sources = cols // (groups * part)
        at = (lax.rem(x, count) * halves + c) * sources
        return held[pl.ds(at, sources)].reshape(cols, 2 * width)

    sums = [jnp.zeros((rows, 2 * width), jnp.float32) for _ in range(2)]
    squares = jnp.zeros((rows, cols), jnp.float32)
    for k in range(count):
        for c in range(halves):
            core = lax.rem(place[1] + (halves - c), halves)
            left = parts[k][:, c].reshape(rows, cols)
            wide = left.astype(jnp.float32)
            squares = squares + wide * wide
            sums = [
                value
                + jnp.dot(
                    left,
                    block(held, place[0] + (count - k), core),
                    preferred_element_type=jnp.float32,
                )
                for value, held in zip(sums, assembled)
            ]
    features = count * halves * cols
    row_scale = lax.rsqrt(jnp.sum(squares, axis=1, keepdims=True) / features + epsilon)
    for j, value in enumerate(sums):
        value = value * row_scale
        gate, up = value[:, :width], value[:, width:]
        hidden = (gate / (1.0 + jnp.exp(-gate)) * up).astype(jnp.bfloat16)
        hidden = hidden.reshape(copies, tokens, width)
        for k in range(count):
            out[k, :, :, j * width : (j + 1) * width] = hidden


def hidden_units(own, other, parts):
    copies, _, tokens, _ = parts[0].shape
    _, sources, part, double = own[0].shape
    groups = sum(piece.shape[0] for piece in own)
    width = double // 2
    out = jax.ShapeDtypeStruct((len(parts), copies, tokens, 2 * width), jnp.bfloat16)
    inputs = (*own, *other, *parts)
    held = pltpu.VMEM((sources, groups, part, 2 * width), jnp.bfloat16)
    return pl.pallas_call(
        functools.partial(hidden_kernel, len(own)),
        out_shape=out,
        grid_spec=pltpu.PrefetchScalarGridSpec(
            num_scalar_prefetch=1,
            grid=(1,),
            in_specs=[whole_block(value) for value in inputs],
            out_specs=whole_block(out),
            scratch_shapes=[held, held],
        ),
        compiler_params=vmem(32),
        name="hidden",
    )(position_of("tp_x", "tp_c", "fs_lo", "grp"), *inputs)


def project_kernel(bundles, place, *refs):
    hidden, out, held = refs[-3:]
    groups = held.shape[2]
    count, copies, tokens, depth = hidden.shape
    halves, cols = out.shape[1], out.shape[3]
    width = depth // 2
    for j, pieces in enumerate((refs[:bundles], refs[bundles : 2 * bundles])):
        step = 0
        for piece in pieces:
            for k in range(piece.shape[0]):
                index = lax.rem(place[3] + (groups - step), groups)
                held[:, :, pl.ds(index, 1), :, j * width : (j + 1) * width] = piece[k][
                    :, :, None
                ]
                step += 1
    share = held.shape[1] // halves
    for c in range(halves):
        value = jnp.zeros((copies * tokens, cols), jnp.float32)
        for k in range(count):
            down = held[k, c * share : (c + 1) * share].reshape(cols, depth)
            value = value + lax.dot_general(
                hidden[k].reshape(copies * tokens, depth),
                down,
                (((1,), (1,)), ((), ())),
                preferred_element_type=jnp.float32,
            )
        value = value.astype(jnp.bfloat16)
        for r in range(copies):
            target = place[2] ^ r
            out[pl.ds(target, 1), c] = value[r * tokens : (r + 1) * tokens][None]


def projected(own, other, hidden, halves):
    _, copies, tokens, depth = hidden.shape
    _, count, sources, part, _ = own[0].shape
    groups = sum(piece.shape[0] for piece in own)
    cols = sources * groups * part // halves
    out = jax.ShapeDtypeStruct((copies, halves, tokens, cols), jnp.bfloat16)
    inputs = (*own, *other, hidden)
    return pl.pallas_call(
        functools.partial(project_kernel, len(own)),
        out_shape=out,
        grid_spec=pltpu.PrefetchScalarGridSpec(
            num_scalar_prefetch=1,
            grid=(1,),
            in_specs=[whole_block(value) for value in inputs],
            out_specs=whole_block(out),
            scratch_shapes=[pltpu.VMEM((count, sources, groups, part, depth), jnp.bfloat16)],
        ),
        compiler_params=vmem(32),
        name="project",
    )(position_of("tp_x", "tp_c", "fs_lo", "grp"), *inputs)


def whole_block(value):
    return pl.BlockSpec(value.shape, lambda t, place, rank=len(value.shape): (0,) * rank)


def choose_kernel(routes, out):
    top, slots, count = out.shape
    capacity = count * 5 // 16
    expert = lax.broadcasted_iota(jnp.int32, (slots // capacity, count), 0)
    named = [routes[k : k + 1, :] == expert for k in range(top)]
    either = functools.reduce(jnp.logical_or, named)
    position = jnp.dot(
        jnp.where(either, 1.0, 0.0).astype(jnp.bfloat16),
        before_matrix(count),
        preferred_element_type=jnp.float32,
    ).astype(jnp.int32)
    slot = lax.broadcasted_iota(jnp.int32, (slots, count), 0)
    for k in range(top):
        mine = jnp.sum(
            jnp.where(named[k], expert * capacity + position, 0), axis=0, keepdims=True
        )
        out[k] = jnp.where(mine == slot, 1.0, 0.0).astype(jnp.bfloat16)


def chosen_slots(routes, slots):
    count, top = routes.shape
    return pl.pallas_call(
        choose_kernel,
        out_shape=jax.ShapeDtypeStruct((top, slots, count), jnp.bfloat16),
        compiler_params=vmem(12),
        name="choose",
    )(routes.T)


def combine_kernel(place, chosen, route_weights, returned, out):
    top, slots, _ = chosen.shape
    values = returned[...].reshape(slots, returned.shape[2])
    total = jnp.zeros(out.shape, jnp.float32)
    for k in range(top):
        picked = lax.dot_general(
            chosen[k], values, (((0,), (0,)), ((), ())), preferred_element_type=jnp.float32
        )
        total = total + route_weights[:, k : k + 1] * picked
    out[...] = total.astype(jnp.bfloat16)


def combined(chosen, route_weights, returned):
    out = jax.ShapeDtypeStruct((route_weights.shape[0], returned.shape[2]), jnp.bfloat16)
    inputs = (chosen, route_weights, returned)
    return pl.pallas_call(
        combine_kernel,
        out_shape=out,
        grid_spec=pltpu.PrefetchScalarGridSpec(
            num_scalar_prefetch=1,
            grid=(1,),
            in_specs=[whole_block(value) for value in inputs],
            out_specs=whole_block(out),
        ),
        compiler_params=vmem(12),
        name="combine",
    )(position_of("grp"), *inputs)


def assembled_weights(pieces, rows):
    groups = len(pieces)
    sources, part, triple = pieces[0].shape
    weights = jnp.zeros((sources, groups, part, triple), jnp.bfloat16)
    for k, piece in enumerate(pieces):
        weights = lax.dynamic_update_slice_in_dim(
            weights, piece[:, None], lax.rem(lax.axis_index("grp") + groups - k, groups), axis=1
        )
    return weights.reshape(sources * rows, triple)


def split_kernel(mine, scaled, down):
    cut = scaled.shape[2]
    scaled[...] = mine[:, :, :cut]
    down[...] = mine[:, :, cut:]


def split_weights(mine):
    sources, part, triple = mine.shape
    cut = 2 * triple // 3
    step = sources // 4

    def spec(width):
        return pl.BlockSpec((step, part, width), lambda t: (t, 0, 0))

    return pl.pallas_call(
        split_kernel,
        out_shape=[
            jax.ShapeDtypeStruct((sources, part, width), jnp.bfloat16)
            for width in (cut, triple - cut)
        ],
        grid=(4,),
        in_specs=[spec(triple)],
        out_specs=[spec(cut), spec(triple - cut)],
        compiler_params=vmem(8),
        name="split",
    )(mine)


def passed_on(value):
    passed = [shifted(value, "grp", k) for k in range(1, lax.axis_size("grp"))]
    pieces = [value[None]] + ([jnp.stack(passed)] if passed else [])
    pairs = []
    for piece in pieces:
        pairs.append(shifted(piece, "tp_c", 1))
    return pieces, pairs


def halved(blocks):
    copies, slots, cols = blocks.shape
    cores = lax.axis_size("tp_c")
    blocks = blocks.reshape(copies, cores, slots // cores, cols)
    halves = []
    for j in range(cores):
        half = lax.dynamic_index_in_dim(
            blocks, lax.rem(lax.axis_index("tp_c") + j, cores), axis=1, keepdims=False
        )
        halves.append(half if j == 0 else shifted(half, "tp_c", j))
    return jnp.stack(halves, axis=1)


def on_device(tokens, routes, route_weights, norm_gain, gate_weight, up_weight, down_weight):
    experts, rows, _ = gate_weight.shape
    copies = lax.axis_size("fs_lo")
    row_count, col_width = tokens.shape
    capacity = row_count * 5 // 16

    outgoing = dispatched(tokens, routes, experts, capacity)
    arrived = exchange(outgoing, "fs_hi")
    block = arrived.reshape(experts * capacity, col_width)
    blocks = [block] + [paired(block, "fs_lo", k) for k in range(1, copies)]
    blocks = halved(jnp.stack(blocks))
    parts = [blocks] + [
        shifted(blocks, "tp_x", k) for k in range(1, lax.axis_size("tp_x"))
    ]

    packed = packed_weights(norm_gain, gate_weight, up_weight, down_weight, copies)
    mine = exchange(packed, FS)
    scaled, down = split_weights(mine)
    turned = exchange(down.reshape(lax.axis_size("tp_x"), -1, *down.shape[1:]), "tp_x")
    scaled, scaled_pairs = passed_on(scaled)
    turned, turned_pairs = passed_on(turned)
    downs = [down] + [shifted(down, "grp", k) for k in range(1, lax.axis_size("grp"))]
    chosen = chosen_slots(routes, experts * capacity)

    units = hidden_units(scaled, scaled_pairs, parts)
    units = exchange(units, "tp_x")
    over_x = projected(turned, turned_pairs, units, lax.axis_size("tp_c"))
    sent = exchange(over_x.reshape(-1, *over_x.shape[2:]), ("fs_lo", "tp_c"))
    over_s = jnp.sum(sent.reshape(over_x.shape), axis=0, dtype=jnp.float32)
    back = over_s.astype(jnp.bfloat16).reshape(experts, capacity, col_width)
    returned = exchange(back, "fs_hi")
    double = assembled_weights([piece for group in scaled for piece in group], rows)
    width = double.shape[1] // 2
    outputs = [double[None, :, :width], double[None, :, width:]]
    outputs.append(assembled_weights(downs, rows)[None])
    return (*outputs, combined(chosen, route_weights, returned))


def solution(mesh):
    split = Mesh(
        mesh.devices.reshape(mesh.shape["grp"], mesh.shape["fs"] // 4, 4, 4, 2),
        ("grp", *FS, *TP),
    )
    rows = P(("grp", *FS), None)
    weight = P(None, FS, TP)
    taken = P(FS, "grp", TP)

    return jax.shard_map(
        on_device,
        mesh=split,
        in_specs=(P(("grp", *FS), TP), rows, rows, P(FS), weight, weight, weight),
        out_specs=(taken, taken, taken, P(("grp", *FS), TP)),
        check_vma=False,
    )
```
